128 devices in a mesh: st: 64 (over z, y, x), tp: 2 (over core).
Axes of the slice: x: 4, y: 4, z: 4, core: 2. Of those that a mesh axis runs over, the one named last changes fastest.
Arguments:
- tokens: bfloat16 [65536, 2048], P('st', 'tp'), may hold values from -6 to 6
- norm_gain: float32 [2048], replicated, may hold values from 0.1 to 1.9
- branch_outer: bfloat16 [2048, 2048], P(None, 'tp'), may hold values from -0.125 to 0.125
- branch_gate: bfloat16 [2048, 2048], P(None, 'tp'), may hold values from -0.125 to 0.125
- branch_input: bfloat16 [2048, 2048], P(None, 'tp'), may hold values from -0.125 to 0.125
- conv_taps: float32 [3, 2048], P(None, 'tp'), may hold values from -3.5 to 3.5
- query_weight: bfloat16 [2048, 1024], P(None, 'tp'), may hold values from -0.125 to 0.125
- query_gain: float32 [128], replicated, may hold values from 0.1 to 1.9
- head_scale: float32 [8], P('tp'), may hold values from 1 to 240
- store: bfloat16 [1024, 64, 2048], P('st'), may hold values from -6 to 6
- store_gain: float32 [2048], replicated, may hold values from 0.1 to 1.9
- key_weight: bfloat16 [2048, 256], P(None, 'tp'), may hold values from -0.125 to 0.125
- value_weight: bfloat16 [2048, 256], P(None, 'tp'), may hold values from -0.125 to 0.125
- key_gain: float32 [128], replicated, may hold values from 0.1 to 1.9
- out_weight: bfloat16 [1024, 2048], P(None, 'tp'), may hold values from -0.1875 to 0.1875
- gate_logit: float32 [2048], P('tp'), may hold values from -1 to 4
- passage_ids: int32 [1024, 4], P('st'), may hold values from 0 to 1023, as said below
Outputs:
- mixed: bfloat16 [65536, 2048], P('st', 'tp')
The draws below stay inside these ranges and needn't reach their ends.
Inputs may be any that keep to these rules, and one draw needn't show every extreme that they name: `passage_ids`: passage p lies in the rows of store held by index p // 16 of st. Among the ids of the rows of one device (its 16 blocks), at most 2 name passages held by any one device, and exactly 2 name passages of some one device; each device names a passage of the device before it and one of the device half the axis away.
All inputs are finite; a program needn't handle non-finite values.
Results may differ from the reference program's by a relative error of at most 0.006.
The reference program's roundings to bfloat16 on the way count: a program that leaves them out, or rounds other values in their place, can miss the bound.
Values may be sent and summed in bfloat16 or wider, within the bound.
A program may use at most 128 MiB of HBM per device.

```python
import math
import jax
import jax.numpy as jnp
from jax import lax

D = 2048
HEADS = 8
KV_HEADS = 2
HEAD_DIM = 128
SEQ = 128
BLK = 64
PB = 4
PLEN = 64
TOK_DEV = 1024
PDEV = 16
TOKENS = 65536
PASSAGES = 1024
N_ST = 64


def draw_head_scale(key, part):
    first_key = jax.random.fold_in(jax.random.fold_in(key, 29), 0)
    scales = jnp.exp(jax.random.uniform(first_key, (HEADS,), jnp.float32, math.log(1.0), math.log(4.0)))
    return scales.astype(jnp.float32)


def draw_passage_ids(key, part):
    requests = TOK_DEV // BLK * PB
    capacity = max(2, (requests + N_ST - 1) // N_ST)
    slots = N_ST * capacity

    def one_device(device):
        device_key = jax.random.fold_in(jax.random.fold_in(key, 17), device)
        keys_list = jax.random.split(device_key, 5)
        slot_order = jnp.arange(slots, dtype=jnp.int32)
        scores = jax.random.randint(keys_list[0], (slots,), 0, 1 << 20) * slots + slot_order
        owners = slot_order // capacity
        ranks = slot_order % capacity
        filled = jax.random.randint(keys_list[1], (), 0, N_ST)
        before = (device - 1) % N_ST
        across = (device + N_ST // 2) % N_ST
        forced = (owners == filled) | ((owners == before) | (owners == across)) & (ranks == 0)
        scores = jnp.where(forced, slot_order - slots, scores)
        picked = jnp.argsort(scores, stable=True)[:requests].astype(jnp.int32)
        chosen_owner = picked // capacity
        local_index = jnp.minimum(jax.random.randint(keys_list[2], (requests,), 0, PDEV), jax.random.randint(keys_list[3], (requests,), 0, PDEV))
        ids = chosen_owner * PDEV + local_index
        shuffle = jax.random.permutation(keys_list[4], requests)
        return ids[shuffle].reshape(requests // PB, PB)
    every = jax.vmap(one_device)(jnp.arange(N_ST, dtype=jnp.int32))
    return every.reshape(N_ST * (TOK_DEV // BLK), PB).astype(jnp.int32)


def level_of(stream_key, extent, cuts, low, largest):
    def one(axis_at, blocks):
        heights = jax.random.uniform(jax.random.fold_in(jax.random.fold_in(stream_key, 6), axis_at), (blocks,), jnp.float32, low / len(cuts), largest / len(cuts))
        return jnp.repeat(jnp.exp(heights), extent[axis_at] // blocks).reshape((-1,) + (1,) * (len(extent) - axis_at - 1))

    level = one(*cuts[0])
    for cut in cuts[1:]:
        level = level * one(*cut)
    return level


def gaussian(key, extent, width, bound, shards=(), kind=jnp.bfloat16):
    loudness = level_of(key, extent, shards, -0.22, 0.18) if shards else 1.0
    array = jax.random.normal(key, extent, jnp.float32) * width * loudness
    return jnp.minimum(jnp.maximum(array, -bound), bound).astype(kind)


def setup_inputs(seed: int = 0) -> dict:
    splits = jax.random.split(jax.random.key(seed), 18)
    tokens = gaussian(splits[0], (TOKENS, D), 1.0, 6.0, ((0, 64), (1, 2)))
    norm_gain = jnp.clip(1.0 + 0.18 * jax.random.normal(splits[1], (D,), jnp.float32), 0.1, 1.9)
    branch_outer = gaussian(splits[2], (D, D), D ** -0.5, 0.125, ((1, 2),))
    branch_gate = gaussian(splits[3], (D, D), D ** -0.5, 0.125, ((1, 2),))
    branch_input = gaussian(splits[4], (D, D), D ** -0.5, 0.125, ((1, 2),))
    conv_taps = gaussian(splits[5], (3, D), 3 ** -0.5, 3.5, ((1, 2),), jnp.float32)
    query_weight = gaussian(splits[6], (D, HEADS * HEAD_DIM), D ** -0.5, 0.125, ((1, 2),))
    query_gain = jnp.clip(1.0 + 0.18 * jax.random.normal(splits[7], (HEAD_DIM,), jnp.float32), 0.1, 1.9)
    head_scale = draw_head_scale(jax.random.fold_in(splits[17], 71), 0)
    store = gaussian(splits[9], (PASSAGES, PLEN, D), 1.0, 6.0, ((0, 64),))
    store_gain = jnp.clip(1.0 + 0.18 * jax.random.normal(splits[10], (D,), jnp.float32), 0.1, 1.9)
    key_weight = gaussian(splits[11], (D, KV_HEADS * HEAD_DIM), D ** -0.5, 0.125, ((1, 2),))
    value_weight = gaussian(splits[12], (D, KV_HEADS * HEAD_DIM), D ** -0.5, 0.125, ((1, 2),))
    key_gain = jnp.clip(1.0 + 0.18 * jax.random.normal(splits[13], (HEAD_DIM,), jnp.float32), 0.1, 1.9)
    out_weight = gaussian(splits[14], (HEADS * HEAD_DIM, D), (HEADS * HEAD_DIM) ** -0.5, 0.1875, ((1, 2),))
    gate_logit = jnp.clip(-1.0 + 5.0 * jax.random.uniform(splits[15], (D,), jnp.float32) ** level_of(splits[15], (D,), ((0, 2),), -0.2, 0.2), -1.0, 4.0)
    passage_ids = draw_passage_ids(jax.random.fold_in(splits[17], 71), 0)
    return dict(tokens=tokens, norm_gain=norm_gain, branch_outer=branch_outer, branch_gate=branch_gate, branch_input=branch_input, conv_taps=conv_taps, query_weight=query_weight, query_gain=query_gain, head_scale=head_scale, store=store, store_gain=store_gain, key_weight=key_weight, value_weight=value_weight, key_gain=key_gain, out_weight=out_weight, gate_logit=gate_logit, passage_ids=passage_ids)


EPS = 1e-06

def norm_rows(values, gain):
    values = values.astype(jnp.float32)
    return values * lax.rsqrt(lax.optimization_barrier(jnp.mean(values * values, axis=-1, keepdims=True)) + EPS) * gain.astype(jnp.float32)

def causal_taps(product, conv_taps):
    token_rows, model_width = product.shape
    grouped = product.reshape(token_rows // SEQ, SEQ, model_width)
    padded = jnp.pad(grouped, ((0, 0), (2, 0), (0, 0)))
    summed = padded[:, 0:SEQ] * conv_taps[0] + padded[:, 1:SEQ + 1] * conv_taps[1] + padded[:, 2:SEQ + 2] * conv_taps[2]
    return summed.reshape(token_rows, model_width)

def passage_partials(queries, key_rows, value_rows):
    scores = jnp.einsum('nqgrd,nkgd->ngrqk', queries.astype(jnp.float32), key_rows.astype(jnp.float32))
    maxima = lax.optimization_barrier(jnp.max(scores, axis=-1))
    weights = jnp.exp(scores - maxima[..., None])
    totals = lax.optimization_barrier(jnp.sum(weights, axis=-1))
    shares = (weights / totals[..., None]).astype(jnp.bfloat16)
    partial_value = jnp.einsum('ngrqk,nkgd->nqgrd', shares.astype(jnp.float32), value_rows.astype(jnp.float32)).astype(jnp.bfloat16)
    return (partial_value, maxima, totals)

def combine_passages(partial_value, maxima, totals):
    highest = lax.optimization_barrier(jnp.max(maxima, axis=1, keepdims=True))
    weight = jnp.exp(maxima - highest) * totals
    denominator = lax.optimization_barrier(jnp.sum(weight, axis=1))
    weight = jnp.transpose(weight, (0, 1, 4, 2, 3))
    summed = lax.optimization_barrier(jnp.sum(partial_value.astype(jnp.float32) * weight[..., None], axis=1))
    return summed / jnp.transpose(denominator, (0, 3, 1, 2))[..., None]

def reference(tokens, norm_gain, branch_outer, branch_gate, branch_input, conv_taps, query_weight, query_gain, head_scale, store, store_gain, key_weight, value_weight, key_gain, out_weight, gate_logit, passage_ids):
    normed = norm_rows(tokens, norm_gain).astype(jnp.bfloat16)
    gate_outer = jnp.dot(normed, branch_outer, preferred_element_type=jnp.float32)
    gate_inner = jnp.dot(normed, branch_gate, preferred_element_type=jnp.float32)
    conv_input = jnp.dot(normed, branch_input, preferred_element_type=jnp.float32)
    conv_out = gate_outer * causal_taps(gate_inner * conv_input, conv_taps.astype(jnp.float32))
    token_rows = tokens.shape[0]
    repeat = HEADS // KV_HEADS
    raw_query = jnp.dot(normed, query_weight, preferred_element_type=jnp.float32).reshape(token_rows, HEADS, HEAD_DIM)
    queries = (norm_rows(raw_query, query_gain) * (head_scale[:, None] / math.sqrt(HEAD_DIM))).astype(jnp.bfloat16)
    queries = queries.reshape(token_rows // BLK, BLK, KV_HEADS, repeat, HEAD_DIM)
    memory = norm_rows(store.reshape(PASSAGES * PLEN, D), store_gain).astype(jnp.bfloat16)
    raw_key = jnp.dot(memory, key_weight, preferred_element_type=jnp.float32).reshape(PASSAGES * PLEN, KV_HEADS, HEAD_DIM)
    key_rows = norm_rows(raw_key, key_gain).astype(jnp.bfloat16).reshape(PASSAGES, PLEN, KV_HEADS, HEAD_DIM)
    value_rows = jnp.dot(memory, value_weight, preferred_element_type=jnp.float32).astype(jnp.bfloat16)
    value_rows = value_rows.reshape(PASSAGES, PLEN, KV_HEADS, HEAD_DIM)

    def one_block(pieces):
        block_query, chosen = pieces
        asked_query = jnp.broadcast_to(block_query[None], (PB,) + block_query.shape)
        return passage_partials(asked_query, key_rows[chosen], value_rows[chosen])
    partial_value, maxima, totals = lax.map(one_block, (queries, passage_ids))
    attended = combine_passages(partial_value, maxima, totals).astype(jnp.bfloat16).reshape(token_rows, HEADS * HEAD_DIM)
    cross = jnp.dot(attended, out_weight, preferred_element_type=jnp.float32)
    return (conv_out + jax.nn.sigmoid(gate_logit) * cross).astype(jnp.bfloat16)
```

```python
import math

import jax
import jax.numpy as jnp
from jax import lax
from jax.experimental import pallas as pl
from jax.experimental.pallas import tpu as pltpu
from jax.sharding import PartitionSpec as P

MESH = pl.DeviceIdType.MESH
EPS = 1e-06
SEQ = 128
RING = 4
CAP = 2
HD = 128
PLEN = 64
BF = jnp.bfloat16
F32 = jnp.float32

ORDERS = (("z", "y", "x"), ("y", "x", "z"), ("x", "z", "y"))
ROWS = (48, 48, 32)
STRIDE = {"z": RING * RING, "y": RING, "x": 1}
GROUP = ((0,), (1, 2, 3))
OFFS = (1, 3, 2)


def coordinates(st):
    return {"z": st // 16, "y": lax.rem(st // 4, 4), "x": lax.rem(st, 4)}


def shifted(st, moves):
    at = coordinates(st)
    out = 0
    for axis in ("z", "y", "x"):
        out = out + lax.rem(at[axis] + (moves.get(axis, 0) % RING), RING) * STRIDE[axis]
    return out


def position(group, oc, ob):
    return (oc * RING + ob) * CAP if group == 0 else RING * RING * CAP + (oc * RING + ob) * 3 * CAP


PLANE = [
    (z, y, x)
    for z in range(RING)
    for y in range(RING)
    for x in range(RING)
    if (z, y, x) != (0, 0, 0) and min(z, y, x) == 0
]


def rel_index(moves):
    return (moves.get("z", 0) * RING + moves.get("y", 0)) * RING + moves.get("x", 0)


def kernel(
    slots,
    tokens,
    norm_gain,
    w_outer,
    w_gate,
    w_input,
    taps,
    w_query,
    query_gain,
    head_scale,
    store,
    store_gain,
    w_key,
    w_value,
    key_gain,
    w_out,
    gate_logit,
    asked,
    out,
    v_store,
    v_wkv,
    v_mem,
    v_x,
    v_n,
    v_wo,
    v_wg,
    v_wi,
    v_wq,
    v_wout,
    v_q,
    v_conv,
    v_att,
    v_attp,
    v_out,
    v_ask,
    s_ask,
    v_k,
    v_v,
    *rest,
):
    table = [rest[f * 4 : f * 4 + 4] for f in range(3)]
    rest = rest[12:]
    packed = [rest[f * 2 : f * 2 + 2] for f in range(3)]
    rest = rest[6:]
    relay = [rest[f * 2 : f * 2 + 2] for f in range(3)]
    rest = rest[6:]
    final = rest[:3]
    (
        local_sem,
        store_sem,
        out_sem,
        ask_ss,
        ask_rs,
        tok_ss,
        tok_rs,
        a_ss,
        a_rs,
        b_ss,
        b_rs,
        c_ss,
        c_rs,
        att_ss,
        att_rs,
    ) = rest[3:]

    st = lax.axis_index("st")
    tp = lax.axis_index("tp")
    other = 1 - tp
    rows_tok = tokens.shape[0]
    half = tokens.shape[1]
    width = 2 * half
    n_pass = store.shape[0] // PLEN

    store_copies = []
    wk = pltpu.make_async_copy(w_key, v_wkv.at[:, pl.ds(0, HD)], local_sem.at[0])
    wv = pltpu.make_async_copy(w_value, v_wkv.at[:, pl.ds(HD, HD)], local_sem.at[1])
    chunk = 256
    for p in range(4):
        store_copies.append(
            pltpu.make_async_copy(
                store.at[pl.ds(p * chunk, chunk)], v_store.at[pl.ds(p * chunk, chunk)], store_sem.at[p]
            )
        )
    store_copies[0].start()
    wk.start()
    wv.start()
    for p in range(1, 4):
        store_copies[p].start()
    tok_local = pltpu.make_async_copy(tokens, v_x.at[tp], local_sem.at[2])
    tok_local.start()
    weights = []
    for i, (src, dst) in enumerate(
        ((w_query, v_wq), (w_outer, v_wo), (w_gate, v_wg), (w_input, v_wi), (w_out, v_wout))
    ):
        cp = pltpu.make_async_copy(src, dst, local_sem.at[3 + i])
        cp.start()
        weights.append(cp)

    barrier = pltpu.get_barrier_semaphore()
    for z, y, x in PLANE:
        pl.semaphore_signal(
            barrier, inc=1, device_id=(shifted(st, {"z": z, "y": y, "x": x}), tp), device_id_type=MESH
        )
    pl.semaphore_signal(barrier, inc=1, device_id=(st, other), device_id_type=MESH)
    pl.semaphore_wait(barrier, len(PLANE) + 1)

    ask_copies = []
    for i, (z, y, x) in enumerate(PLANE):
        cp = pltpu.make_async_remote_copy(
            src_ref=asked,
            dst_ref=v_ask.at[rel_index({"z": z, "y": y, "x": x})],
            send_sem=ask_ss.at[i],
            recv_sem=ask_rs.at[i],
            device_id=(shifted(st, {"z": -z, "y": -y, "x": -x}), tp),
            device_id_type=MESH,
        )
        cp.start()
        ask_copies.append(cp)
    tok_remote = pltpu.make_async_remote_copy(
        src_ref=tokens,
        dst_ref=v_x.at[tp],
        send_sem=tok_ss,
        recv_sem=tok_rs,
        device_id=(st, other),
        device_id_type=MESH,
    )
    tok_remote.start()
    v_ask[0] = asked[...]

    def a_copy(f, o, p):
        return pltpu.make_async_remote_copy(
            src_ref=table[f][0].at[pl.ds(p * 4, 4)],
            dst_ref=table[f][o].at[pl.ds(p * 4, 4)],
            send_sem=a_ss.at[f * 3 + o - 1, p],
            recv_sem=a_rs.at[f * 3 + o - 1, p],
            device_id=(shifted(st, {ORDERS[f][0]: o}), tp),
            device_id_type=MESH,
        )

    wk.wait()
    wv.wait()
    sub = 32

    def kv_chunk(p, carry):
        base = p * chunk
        pltpu.make_async_copy(
            store.at[pl.ds(base, chunk)], v_store.at[pl.ds(base, chunk)], store_sem.at[p]
        ).wait()

        def norm_sub(i, c):
            x = v_store[pl.ds(base + i * sub, sub), :].astype(F32)
            r = lax.rsqrt(jnp.mean(x * x, axis=-1, keepdims=True) + EPS)
            v_mem[pl.ds(i * sub, sub), :] = (x * r * store_gain[...]).astype(BF)
            return c

        lax.fori_loop(0, chunk // sub, norm_sub, 0, unroll=2)
        kv = jnp.dot(v_mem[...], v_wkv[...], preferred_element_type=F32)
        k = kv[:, :HD]
        k = k * lax.rsqrt(jnp.mean(k * k, axis=-1, keepdims=True) + EPS) * key_gain[...]
        k = k.astype(BF).reshape(4, PLEN, HD)
        v = kv[:, HD:].astype(BF).reshape(4, PLEN, HD)
        at = pl.ds(p * 4, 4)
        table[0][0][at, :, :] = k[:, 0:48]
        table[1][0][at, 0:16, :] = k[:, 48:64]
        table[1][0][at, 16:48, :] = v[:, 0:32]
        table[2][0][at, :, :] = v[:, 32:64]
        for o in OFFS:
            for f in range(3):
                a_copy(f, o, p).start()
        return carry

    lax.fori_loop(0, 4, kv_chunk, 0)

    for cp in ask_copies:
        cp.wait_recv()
    ask_local = pltpu.make_async_copy(v_ask, s_ask, local_sem.at[8])
    ask_local.start()
    ask_local.wait()

    def pack(group):
        n = len(GROUP[group]) * CAP
        for f in range(3):
            aa, ab, ac = ORDERS[f]
            owners = [shifted(st, {aa: -o}) for o in GROUP[group]]

            def one(t, carry, f=f, ab=ab, ac=ac, owners=owners):
                ob = t // RING
                oc = lax.rem(t, RING)
                rel = ob * STRIDE[ab] + oc * STRIDE[ac]
                for j, o in enumerate(GROUP[group]):
                    for r in range(CAP):
                        at = s_ask[rel, 0, owners[j] * CAP + r]
                        packed[f][group][ob, oc, j * CAP + r] = table[f][o][at]
                return carry

            lax.fori_loop(0, RING * RING, one, 0, unroll=2)
            final[f][pl.ds(position(group, 0, 0), n)] = packed[f][group][0, 0]

    def b_copies(f, group, ob):
        n = len(GROUP[group]) * CAP
        to = (shifted(st, {ORDERS[f][1]: ob}), tp)
        i = (f * 2 + group) * 3 + ob - 1
        return (
            pltpu.make_async_remote_copy(
                src_ref=packed[f][group].at[ob, pl.ds(1, 3)],
                dst_ref=relay[f][group].at[ob - 1],
                send_sem=b_ss.at[i, 0],
                recv_sem=b_rs.at[i, 0],
                device_id=to,
                device_id_type=MESH,
            ),
            pltpu.make_async_remote_copy(
                src_ref=packed[f][group].at[ob, 0],
                dst_ref=final[f].at[pl.ds(position(group, 0, ob), n)],
                send_sem=b_ss.at[i, 1],
                recv_sem=b_rs.at[i, 1],
                device_id=to,
                device_id_type=MESH,
            ),
        )

    def c_copy(f, group, oc, ob):
        n = len(GROUP[group]) * CAP
        i = ((f * 2 + group) * 3 + oc - 1) * 4 + ob
        src = packed[f][group].at[0, oc] if ob == 0 else relay[f][group].at[ob - 1, oc - 1]
        return pltpu.make_async_remote_copy(
            src_ref=src,
            dst_ref=final[f].at[pl.ds(position(group, oc, ob), n)],
            send_sem=c_ss.at[i],
            recv_sem=c_rs.at[i],
            device_id=(shifted(st, {ORDERS[f][2]: oc}), tp),
            device_id_type=MESH,
        )

    def send_packed(group):
        for f in range(3):
            for ob in OFFS:
                b_copies(f, group, ob)[0].start()
        for f in range(3):
            for ob in OFFS:
                b_copies(f, group, ob)[1].start()
        for f in range(3):
            for oc in OFFS:
                c_copy(f, group, oc, 0).start()

    def forward(group, ob):
        for f in range(3):
            b_copies(f, group, ob)[0].wait_recv()
            for oc in OFFS:
                c_copy(f, group, oc, ob).start()

    pack(0)
    send_packed(0)

    tok_local.wait()
    tok_remote.wait_recv()

    def norm_tok(i, c):
        at = pl.ds(i * sub, sub)
        x0 = v_x[0, at, :].astype(F32)
        x1 = v_x[1, at, :].astype(F32)
        total = jnp.sum(x0 * x0, axis=-1, keepdims=True) + jnp.sum(x1 * x1, axis=-1, keepdims=True)
        r = lax.rsqrt(total * (1.0 / width) + EPS)
        v_n[at, pl.ds(0, half)] = (x0 * r * norm_gain[:, 0:half]).astype(BF)
        v_n[at, pl.ds(half, half)] = (x1 * r * norm_gain[:, half:width]).astype(BF)
        return c

    lax.fori_loop(0, rows_tok // sub, norm_tok, 0, unroll=2)

    weights[0].wait()
    n_heads = v_q.shape[1]

    def query_chunk(i, c):
        raw = jnp.dot(v_n[pl.ds(i * chunk, chunk), :], v_wq[...], preferred_element_type=F32)
        for h in range(n_heads):
            q = raw[:, h * HD : (h + 1) * HD]
            q = q * lax.rsqrt(jnp.mean(q * q, axis=-1, keepdims=True) + EPS) * query_gain[...]
            q = (q * (head_scale[h] / math.sqrt(HD))).astype(BF).reshape(chunk // PLEN, PLEN, HD)
            v_q[pl.ds(i * (chunk // PLEN), chunk // PLEN), h] = q
        return c

    lax.fori_loop(0, rows_tok // chunk, query_chunk, 0)

    for f in range(3):
        for o in OFFS:
            for p in range(4):
                a_copy(f, o, p).wait_recv()
    pack(1)
    send_packed(1)

    for cp in weights[1:4]:
        cp.wait()
    tall, wide = 512, 256
    cols = v_wo.shape[1] // wide

    def branch(s, carry):
        rows = pl.ds(pl.multiple_of((s // cols) * tall, tall), tall)
        at = pl.ds(pl.multiple_of(lax.rem(s, cols) * wide, wide), wide)
        n = v_n[rows, :]
        gate = jnp.dot(n, v_wg[:, at], preferred_element_type=F32)
        z = gate * jnp.dot(n, v_wi[:, at], preferred_element_type=F32)
        row = lax.rem(lax.broadcasted_iota(jnp.int32, (tall, wide), 0), SEQ)
        one = jnp.where(row >= 1, pltpu.roll(z, 1, 0), 0.0)
        two = jnp.where(row >= 2, pltpu.roll(z, 2, 0), 0.0)
        t = taps[:, at]
        conv = two * t[0:1] + one * t[1:2] + z * t[2:3]
        v_conv[rows, at] = conv
        v_conv[rows, at] = (
            jnp.dot(n, v_wo[:, at], preferred_element_type=F32) * v_conv[rows, at]
        )

        @pl.when(s == 0)
        def _():
            forward(0, 1)
            forward(0, 3)

        @pl.when(s == 1)
        def _():
            forward(0, 2)

        @pl.when(s == 4)
        def _():
            forward(1, 1)
            forward(1, 3)

        @pl.when(s == 6)
        def _():
            forward(1, 2)

        return carry

    lax.fori_loop(0, (rows_tok // tall) * cols, branch, 0)

    weights[4].wait()
    for f in range(3):
        for group in range(2):
            for ob in OFFS:
                b_copies(f, group, ob)[1].wait_recv()
            for oc in OFFS:
                for ob in range(RING):
                    c_copy(f, group, oc, ob).wait_recv()

    n_blocks = v_q.shape[0]
    per_block = 4

    def attend(b, carry):
        for j in range(per_block):
            first = final[0][slots[0, b * per_block + j]]
            second = final[1][slots[1, b * per_block + j]]
            third = final[2][slots[2, b * per_block + j]]
            v_k[pl.ds(j * PLEN, 48), :] = first
            v_k[pl.ds(j * PLEN + 48, 16), :] = second[0:16]
            v_v[pl.ds(j * PLEN, 32), :] = second[16:48]
            v_v[pl.ds(j * PLEN + 32, 32), :] = third
        q = v_q[b].reshape(n_heads * PLEN, HD)
        scores = lax.dot_general(
            q, v_k[...], (((1,), (1,)), ((), ())), preferred_element_type=F32
        )
        top = jnp.max(scores, axis=-1, keepdims=True)
        weight = jnp.exp(scores - top)
        total = jnp.sum(weight, axis=-1, keepdims=True)
        share = (weight / total).astype(BF)
        value = jnp.dot(share, v_v[...], preferred_element_type=F32).astype(BF)
        at = pl.ds(b * PLEN, PLEN)
        for h in range(n_heads):
            v_att[at, pl.ds(h * HD, HD)] = value[h * PLEN : (h + 1) * PLEN]
        return carry

    def att_copy(i):
        return pltpu.make_async_remote_copy(
            src_ref=v_att.at[pl.ds(i * chunk, chunk)],
            dst_ref=v_attp.at[pl.ds(i * chunk, chunk)],
            send_sem=att_ss.at[i],
            recv_sem=att_rs.at[i],
            device_id=(st, other),
            device_id_type=MESH,
        )

    n_chunks = rows_tok // chunk

    def attend_chunk(i, carry):
        per = n_blocks // n_chunks
        lax.fori_loop(i * per, (i + 1) * per, attend, 0)
        att_copy(i).start()
        return carry

    lax.fori_loop(0, n_chunks, attend_chunk, 0)

    mine = v_att.shape[1]

    def out_copy(i):
        at = pl.ds(i * chunk, chunk)
        return pltpu.make_async_copy(v_out.at[at], out.at[at], out_sem.at[i])

    def project(i, carry):
        at = pl.ds(pl.multiple_of(i * chunk, chunk), chunk)
        att_copy(i).wait_recv()
        cross = jnp.dot(
            v_att[at, :], v_wout[pl.ds(pl.multiple_of(tp * mine, mine), mine), :], preferred_element_type=F32
        )
        cross = cross + jnp.dot(
            v_attp[at, :],
            v_wout[pl.ds(pl.multiple_of(other * mine, mine), mine), :],
            preferred_element_type=F32,
        )
        v_out[at, :] = (v_conv[at, :] + jax.nn.sigmoid(gate_logit[...]) * cross).astype(BF)
        out_copy(i).start()
        return carry

    lax.fori_loop(0, n_chunks, project, 0)

    for i in range(n_chunks):
        out_copy(i).wait()
        att_copy(i).wait_send()
    for cp in ask_copies:
        cp.wait_send()
    tok_remote.wait_send()
    for f in range(3):
        for o in OFFS:
            for p in range(4):
                a_copy(f, o, p).wait_send()
        for group in range(2):
            for ob in OFFS:
                for cp in b_copies(f, group, ob):
                    cp.wait_send()
            for oc in OFFS:
                for ob in range(RING):
                    c_copy(f, group, oc, ob).wait_send()


def request_tables(passage_ids, n_pass, n_st):
    flat = passage_ids.reshape(-1)
    requests = flat.shape[0]
    owner = flat // n_pass
    local = flat - owner * n_pass
    order = jnp.arange(requests, dtype=jnp.int32)
    same = (owner[:, None] == owner[None, :]) & (order[None, :] < order[:, None])
    rank = jnp.sum(same.astype(jnp.int32), axis=1)
    match = (owner * CAP + rank)[:, None] == jnp.arange(n_st * CAP, dtype=jnp.int32)[None, :]
    asked = jnp.sum(jnp.where(match, local[:, None], 0), axis=0).reshape(1, n_st * CAP)
    me = coordinates(lax.axis_index("st"))
    them = coordinates(owner)
    rows = []
    for order_f in ORDERS:
        oa, ob, oc = [lax.rem(me[axis] - them[axis] + RING, RING) for axis in order_f]
        spot = oc * RING + ob
        near = spot * CAP + rank
        far = RING * RING * CAP + spot * 3 * CAP + (oa - 1) * CAP + rank
        rows.append(jnp.where(oa == 0, near, far))
    return asked.astype(jnp.int32), jnp.stack(rows).astype(jnp.int32)


def on_device(
    tokens,
    norm_gain,
    branch_outer,
    branch_gate,
    branch_input,
    conv_taps,
    query_weight,
    query_gain,
    head_scale,
    store,
    store_gain,
    key_weight,
    value_weight,
    key_gain,
    out_weight,
    gate_logit,
    passage_ids,
):
    n_pass, plen, width = store.shape
    n_tok, half = tokens.shape
    heads = head_scale.shape[0]
    n_st = lax.axis_size("st")
    asked, slots = request_tables(passage_ids, n_pass, n_st)
    blocks = passage_ids.shape[0]

    vmem = pl.BlockSpec(memory_space=pltpu.VMEM)
    smem = pl.BlockSpec(memory_space=pltpu.SMEM)
    hbm = pl.BlockSpec(memory_space=pl.ANY)
    dma = pltpu.SemaphoreType.DMA
    scratch = [
        pltpu.VMEM((n_pass * plen, width), BF),
        pltpu.VMEM((width, 2 * HD), BF),
        pltpu.VMEM((256, width), BF),
        pltpu.VMEM((2, n_tok, half), BF),
        pltpu.VMEM((n_tok, width), BF),
        pltpu.VMEM(branch_outer.shape, BF),
        pltpu.VMEM(branch_gate.shape, BF),
        pltpu.VMEM(branch_input.shape, BF),
        pltpu.VMEM(query_weight.shape, BF),
        pltpu.VMEM(out_weight.shape, BF),
        pltpu.VMEM((blocks, heads, plen, HD), BF),
        pltpu.VMEM((n_tok, half), F32),
        pltpu.VMEM((n_tok, heads * HD), BF),
        pltpu.VMEM((n_tok, heads * HD), BF),
        pltpu.VMEM((n_tok, half), BF),
        pltpu.VMEM((n_st, 1, n_st * CAP), jnp.int32),
        pltpu.SMEM((n_st, 1, n_st * CAP), jnp.int32),
        pltpu.VMEM((4 * plen, HD), BF),
        pltpu.VMEM((4 * plen, HD), BF),
    ]
    for f in range(3):
        scratch += [pltpu.VMEM((n_pass, ROWS[f], HD), BF)] * RING
    for f in range(3):
        scratch += [pltpu.VMEM((RING, RING, len(g) * CAP, ROWS[f], HD), BF) for g in GROUP]
    for f in range(3):
        scratch += [pltpu.VMEM((3, 3, len(g) * CAP, ROWS[f], HD), BF) for g in GROUP]
    for f in range(3):
        scratch += [pltpu.VMEM((n_st * CAP, ROWS[f], HD), BF)]
    scratch += [
        dma((9,)),
        dma((4,)),
        dma((4,)),
        dma((len(PLANE),)),
        dma((len(PLANE),)),
        dma,
        dma,
        dma((9, 4)),
        dma((9, 4)),
        dma((18, 2)),
        dma((18, 2)),
        dma((72,)),
        dma((72,)),
        dma((4,)),
        dma((4,)),
    ]
    return pl.pallas_call(
        kernel,
        out_shape=jax.ShapeDtypeStruct((n_tok, half), BF),
        in_specs=[
            smem,
            hbm,
            vmem,
            hbm,
            hbm,
            hbm,
            vmem,
            hbm,
            vmem,
            smem,
            hbm,
            vmem,
            hbm,
            hbm,
            vmem,
            hbm,
            vmem,
            vmem,
        ],
        out_specs=hbm,
        scratch_shapes=scratch,
        compiler_params=pltpu.CompilerParams(
            collective_id=0, has_side_effects=True, vmem_limit_bytes=62 * 1024 * 1024
        ),
    )(
        slots,
        tokens,
        norm_gain.reshape(1, -1),
        branch_outer,
        branch_gate,
        branch_input,
        conv_taps,
        query_weight,
        query_gain.reshape(1, -1),
        head_scale,
        store.reshape(n_pass * plen, width),
        store_gain.reshape(1, -1),
        key_weight,
        value_weight,
        key_gain.reshape(1, -1),
        out_weight,
        gate_logit.reshape(1, -1),
        asked,
    )


def solution(mesh):
    return jax.shard_map(
        on_device,
        mesh=mesh,
        in_specs=(
            P("st", "tp"),
            P(),
            P(None, "tp"),
            P(None, "tp"),
            P(None, "tp"),
            P(None, "tp"),
            P(None, "tp"),
            P(),
            P("tp"),
            P("st", None, None),
            P(),
            P(None, "tp"),
            P(None, "tp"),
            P(),
            P(None, "tp"),
            P("tp"),
            P("st", None),
        ),
        out_specs=P("st", "tp"),
        check_vma=False,
    )
```

```python
import math

import jax
import jax.numpy as jnp
from jax import lax
from jax.experimental import pallas as pl
from jax.experimental.pallas import tpu as pltpu
from jax.sharding import PartitionSpec as P

MESH = pl.DeviceIdType.MESH
EPS = 1e-06
SEQ = 128
RING = 4
CAP = 2
HD = 128
PLEN = 64
BF = jnp.bfloat16
F32 = jnp.float32

ORDERS = (("z", "y", "x"), ("y", "x", "z"), ("x", "z", "y"))
ROWS = (48, 48, 32)
STRIDE = {"z": RING * RING, "y": RING, "x": 1}
GROUP = ((0,), (1, 2, 3))
OFFS = (1, 3, 2)


def coordinates(st):
    return {"z": st // 16, "y": lax.rem(st // 4, 4), "x": lax.rem(st, 4)}


def shifted(st, moves):
    at = coordinates(st)
    out = 0
    for axis in ("z", "y", "x"):
        out = out + lax.rem(at[axis] + (moves.get(axis, 0) % RING), RING) * STRIDE[axis]
    return out


def position(group, oc, ob):
    return (oc * RING + ob) * CAP if group == 0 else RING * RING * CAP + (oc * RING + ob) * 3 * CAP


def kernel(
    ids,
    tokens,
    norm_gain,
    w_outer,
    w_gate,
    w_input,
    taps,
    w_query,
    query_gain,
    head_scale,
    store,
    store_gain,
    w_key,
    w_value,
    key_gain,
    w_out,
    gate_logit,
    out,
    v_store,
    v_wkv,
    v_mem,
    v_x,
    v_n,
    v_wo,
    v_wg,
    v_wi,
    v_wq,
    v_wout,
    v_q,
    v_conv,
    v_att,
    v_attp,
    v_out,
    v_ask,
    s_ask,
    v_put,
    v_slots,
    s_slots,
    *rest,
):
    table = [rest[f * 4 : f * 4 + 4] for f in range(3)]
    rest = rest[12:]
    packed = [rest[f * 2 : f * 2 + 2] for f in range(3)]
    rest = rest[6:]
    relay = [rest[f * 2 : f * 2 + 2] for f in range(3)]
    rest = rest[6:]
    final = rest[:3]
    (
        local_sem,
        store_sem,
        out_sem,
        ask_ss,
        ask_rs,
        tok_ss,
        tok_rs,
        a_ss,
        a_rs,
        b_ss,
        b_rs,
        c_ss,
        c_rs,
        att_ss,
        att_rs,
    ) = rest[3:]

    st = lax.axis_index("st")
    tp = lax.axis_index("tp")
    other = 1 - tp
    rows_tok = tokens.shape[0]
    half = tokens.shape[1]
    width = 2 * half
    n_pass = store.shape[0] // PLEN

    store_copies = []
    wk = pltpu.make_async_copy(w_key, v_wkv.at[:, pl.ds(0, HD)], local_sem.at[0])
    wv = pltpu.make_async_copy(w_value, v_wkv.at[:, pl.ds(HD, HD)], local_sem.at[1])
    chunk = 256
    for p in range(4):
        store_copies.append(
            pltpu.make_async_copy(
                store.at[pl.ds(p * chunk, chunk)], v_store.at[pl.ds(p * chunk, chunk)], store_sem.at[p]
            )
        )
    store_copies[0].start()
    wk.start()
    wv.start()
    for p in range(1, 4):
        store_copies[p].start()
    tok_local = pltpu.make_async_copy(tokens, v_x.at[tp], local_sem.at[2])
    tok_local.start()
    weights = []
    for i, (src, dst) in enumerate(
        ((w_query, v_wq), (w_outer, v_wo), (w_gate, v_wg), (w_input, v_wi), (w_out, v_wout))
    ):
        cp = pltpu.make_async_copy(src, dst, local_sem.at[3 + i])
        cp.start()
        weights.append(cp)

    barrier = pltpu.get_barrier_semaphore()
    for axis in STRIDE:
        for o in OFFS:
            pl.semaphore_signal(barrier, inc=1, device_id=(shifted(st, {axis: o}), tp), device_id_type=MESH)
    pl.semaphore_signal(barrier, inc=1, device_id=(st, other), device_id_type=MESH)

    lanes = v_put.shape[1]
    lane = lax.broadcasted_iota(jnp.int32, (1, lanes), 1)
    lane_owner = lane // CAP
    lane_rank = lax.rem(lane, CAP)
    per_block, n_blocks = ids.shape
    v_put[...] = jnp.zeros_like(v_put)

    def request(j, carry):
        wanted, count = carry
        for p in range(per_block):
            number = ids[p, j]
            owner = lax.div(number, n_pass)
            match = lane_owner == owner
            put = match & (count == lane_rank)
            wanted = jnp.where(put, number - owner * n_pass, wanted)
            count = count + match.astype(jnp.int32)
            v_put[pl.ds(j * per_block + p, 1), :] = put.astype(jnp.int32)
        return wanted, count

    zero = jnp.zeros((1, lanes), jnp.int32)
    wanted, _ = lax.fori_loop(0, n_blocks, request, (zero, zero), unroll=4)
    for f in range(3):
        v_ask[f, 0, 0] = wanted
    me = coordinates(st)
    them = {
        "z": lane_owner // (RING * RING),
        "y": lax.rem(lane_owner // RING, RING),
        "x": lax.rem(lane_owner, RING),
    }
    for f in range(3):
        oa, ob, oc = [lax.rem(me[axis] - them[axis] + RING, RING) for axis in ORDERS[f]]
        spot = oc * RING + ob
        near = spot * CAP + lane_rank
        far = RING * RING * CAP + spot * 3 * CAP + (oa - 1) * CAP + lane_rank
        spots = v_put[...] * jnp.where(oa == 0, near, far)
        v_slots[f] = jnp.sum(spots.T, axis=0, keepdims=True)

    def ask_first(f, oc):
        return pltpu.make_async_remote_copy(
            src_ref=v_ask.at[f, 0, 0],
            dst_ref=v_ask.at[f, 0, oc],
            send_sem=ask_ss.at[f, oc - 1],
            recv_sem=ask_rs.at[f, oc - 1],
            device_id=(shifted(st, {ORDERS[f][2]: -oc}), tp),
            device_id_type=MESH,
        )

    def ask_second(f, ob):
        return pltpu.make_async_remote_copy(
            src_ref=v_ask.at[f, 0],
            dst_ref=v_ask.at[f, ob],
            send_sem=ask_ss.at[f, 2 + ob],
            recv_sem=ask_rs.at[f, 2 + ob],
            device_id=(shifted(st, {ORDERS[f][1]: -ob}), tp),
            device_id_type=MESH,
        )

    tok_remote = pltpu.make_async_remote_copy(
        src_ref=tokens,
        dst_ref=v_x.at[tp],
        send_sem=tok_ss,
        recv_sem=tok_rs,
        device_id=(st, other),
        device_id_type=MESH,
    )

    def a_copy(f, o, p):
        ahead = o == 1 or (o == 2 and p < 2)
        src = table[f][0] if o != 2 else table[f][1 if ahead else 3]
        return a_step(f, o, p, src, 1 if ahead else 3)

    def a_step(f, o, p, src, move):
        return pltpu.make_async_remote_copy(
            src_ref=src.at[pl.ds(p * 4, 4)],
            dst_ref=table[f][o].at[pl.ds(p * 4, 4)],
            send_sem=a_ss.at[f * 3 + o - 1, p],
            recv_sem=a_rs.at[f * 3 + o - 1, p],
            device_id=(shifted(st, {ORDERS[f][0]: move}), tp),
            device_id_type=MESH,
        )

    wk.wait()
    wv.wait()
    sub = 32

    def kv_chunk(p, carry):
        base = p * chunk
        pltpu.make_async_copy(
            store.at[pl.ds(base, chunk)], v_store.at[pl.ds(base, chunk)], store_sem.at[p]
        ).wait()

        def norm_sub(i, c):
            x = v_store[pl.ds(base + i * sub, sub), :].astype(F32)
            r = lax.rsqrt(jnp.mean(x * x, axis=-1, keepdims=True) + EPS)
            v_mem[pl.ds(i * sub, sub), :] = (x * r * store_gain[...]).astype(BF)
            return c

        lax.fori_loop(0, chunk // sub, norm_sub, 0, unroll=2)
        kv = jnp.dot(v_mem[...], v_wkv[...], preferred_element_type=F32)
        k = kv[:, :HD]
        k = k * lax.rsqrt(jnp.mean(k * k, axis=-1, keepdims=True) + EPS) * key_gain[...]
        k = k.astype(BF).reshape(4, PLEN, HD)
        v = kv[:, HD:].astype(BF).reshape(4, PLEN, HD)
        at = pl.ds(p * 4, 4)
        table[0][0][at, :, :] = k[:, 0:48]
        table[1][0][at, 0:16, :] = k[:, 48:64]
        table[1][0][at, 16:48, :] = v[:, 0:32]
        table[2][0][at, :, :] = v[:, 32:64]

        @pl.when(p == 0)
        def _():
            pl.semaphore_wait(barrier, 3 * len(OFFS) + 1)
            for f in range(3):
                for oc in OFFS:
                    ask_first(f, oc).start()

        for f in range(3):
            for o in (1, 3):
                a_step(f, o, p, table[f][0], o).start()

        @pl.when(p == 0)
        def _():
            tok_remote.start()

        return carry

    lax.fori_loop(0, 4, kv_chunk, 0)

    for f in range(3):
        for oc in OFFS:
            ask_first(f, oc).wait_recv()
    for f in range(3):
        for ob in OFFS:
            ask_second(f, ob).start()

    def pack(group):
        n = len(GROUP[group]) * CAP
        for f in range(3):
            owners = [shifted(st, {ORDERS[f][0]: -o}) for o in GROUP[group]]

            def one(t, carry, f=f, owners=owners):
                ob = t // RING
                oc = lax.rem(t, RING)
                for j, o in enumerate(GROUP[group]):
                    for r in range(CAP):
                        at = s_ask[f, ob, oc, 0, owners[j] * CAP + r]
                        packed[f][group][ob, oc, j * CAP + r] = table[f][o][at]
                return carry

            lax.fori_loop(0, RING * RING, one, 0, unroll=2)
            final[f][pl.ds(position(group, 0, 0), n)] = packed[f][group][0, 0]

    def b_copies(f, group, ob):
        n = len(GROUP[group]) * CAP
        to = (shifted(st, {ORDERS[f][1]: ob}), tp)
        i = (f * 2 + group) * 3 + ob - 1
        return (
            pltpu.make_async_remote_copy(
                src_ref=packed[f][group].at[ob, pl.ds(1, 3)],
                dst_ref=relay[f][group].at[ob - 1],
                send_sem=b_ss.at[i, 0],
                recv_sem=b_rs.at[i, 0],
                device_id=to,
                device_id_type=MESH,
            ),
            pltpu.make_async_remote_copy(
                src_ref=packed[f][group].at[ob, 0],
                dst_ref=final[f].at[pl.ds(position(group, 0, ob), n)],
                send_sem=b_ss.at[i, 1],
                recv_sem=b_rs.at[i, 1],
                device_id=to,
                device_id_type=MESH,
            ),
        )

    def c_copy(f, group, oc, ob):
        n = len(GROUP[group]) * CAP
        i = ((f * 2 + group) * 3 + oc - 1) * 4 + ob
        src = packed[f][group].at[0, oc] if ob == 0 else relay[f][group].at[ob - 1, oc - 1]
        return pltpu.make_async_remote_copy(
            src_ref=src,
            dst_ref=final[f].at[pl.ds(position(group, oc, ob), n)],
            send_sem=c_ss.at[i],
            recv_sem=c_rs.at[i],
            device_id=(shifted(st, {ORDERS[f][2]: oc}), tp),
            device_id_type=MESH,
        )

    def send_packed(group):
        for f in range(3):
            for ob in OFFS:
                b_copies(f, group, ob)[0].start()
        for f in range(3):
            for ob in OFFS:
                b_copies(f, group, ob)[1].start()
        for f in range(3):
            for oc in OFFS:
                c_copy(f, group, oc, 0).start()

    def forward(group, ob):
        for f in range(3):
            b_copies(f, group, ob)[0].wait_recv()
            for oc in OFFS:
                c_copy(f, group, oc, ob).start()

    tok_local.wait()

    def norm_tok(i, c):
        at = pl.ds(i * sub, sub)
        x0 = v_x[0, at, :].astype(F32)
        x1 = v_x[1, at, :].astype(F32)
        total = jnp.sum(x0 * x0, axis=-1, keepdims=True) + jnp.sum(x1 * x1, axis=-1, keepdims=True)
        r = lax.rsqrt(total * (1.0 / width) + EPS)
        v_n[at, pl.ds(0, half)] = (x0 * r * norm_gain[:, 0:half]).astype(BF)
        v_n[at, pl.ds(half, half)] = (x1 * r * norm_gain[:, half:width]).astype(BF)
        return c

    tok_remote.wait_recv()
    n_sub = rows_tok // sub
    lax.fori_loop(0, n_sub // 2, norm_tok, 0, unroll=2)

    for f in range(3):
        for p in range(4):
            o = 1 if p < 2 else 3
            a_copy(f, o, p).wait_recv()
            a_copy(f, 2, p).start()
    for f in range(3):
        for ob in OFFS:
            ask_second(f, ob).wait_recv()
    ask_local = pltpu.make_async_copy(v_ask, s_ask, local_sem.at[8])
    ask_local.start()
    slots_local = pltpu.make_async_copy(v_slots, s_slots, local_sem.at[9])
    slots_local.start()
    ask_local.wait()
    slots_local.wait()
    pack(0)
    send_packed(0)
    lax.fori_loop(n_sub // 2, n_sub, norm_tok, 0, unroll=2)

    weights[0].wait()
    n_heads = v_q.shape[1]

    def query_chunk(i, c):
        raw = jnp.dot(v_n[pl.ds(i * chunk, chunk), :], v_wq[...], preferred_element_type=F32)
        for h in range(n_heads):
            q = raw[:, h * HD : (h + 1) * HD]
            q = q * lax.rsqrt(jnp.mean(q * q, axis=-1, keepdims=True) + EPS) * query_gain[...]
            q = (q * (head_scale[h] / math.sqrt(HD))).astype(BF).reshape(chunk // PLEN, PLEN, HD)
            v_q[pl.ds(i * (chunk // PLEN), chunk // PLEN), h] = q
        return c

    lax.fori_loop(0, rows_tok // chunk, query_chunk, 0)

    for f in range(3):
        for p in range(4):
            a_copy(f, 3 if p < 2 else 1, p).wait_recv()
            a_copy(f, 2, p).wait_recv()
    pack(1)
    send_packed(1)

    for cp in weights[1:4]:
        cp.wait()
    tall, wide = 512, 256
    cols = v_wo.shape[1] // wide

    def branch(s, carry):
        rows = pl.ds(pl.multiple_of((s // cols) * tall, tall), tall)
        at = pl.ds(pl.multiple_of(lax.rem(s, cols) * wide, wide), wide)
        n = v_n[rows, :]
        gate = jnp.dot(n, v_wg[:, at], preferred_element_type=F32)
        z = gate * jnp.dot(n, v_wi[:, at], preferred_element_type=F32)
        row = lax.rem(lax.broadcasted_iota(jnp.int32, (tall, wide), 0), SEQ)
        one = jnp.where(row >= 1, pltpu.roll(z, 1, 0), 0.0)
        two = jnp.where(row >= 2, pltpu.roll(z, 2, 0), 0.0)
        t = taps[:, at]
        conv = two * t[0:1] + one * t[1:2] + z * t[2:3]
        v_conv[rows, at] = conv
        v_conv[rows, at] = (
            jnp.dot(n, v_wo[:, at], preferred_element_type=F32) * v_conv[rows, at]
        )

        @pl.when(s == 0)
        def _():
            forward(0, 1)
            forward(0, 3)

        @pl.when(s == 1)
        def _():
            forward(0, 2)

        @pl.when(s == 4)
        def _():
            forward(1, 1)
            forward(1, 3)

        @pl.when(s == 6)
        def _():
            forward(1, 2)

        return carry

    lax.fori_loop(0, (rows_tok // tall) * cols, branch, 0)

    weights[4].wait()
    for f in range(3):
        for group in range(2):
            for ob in OFFS:
                b_copies(f, group, ob)[1].wait_recv()
            for oc in OFFS:
                for ob in range(RING):
                    c_copy(f, group, oc, ob).wait_recv()

    heads_rows = n_heads * PLEN
    ones = jnp.ones((per_block * PLEN, HD), BF)

    def attend(b):
        keys, values = [], []
        for j in range(per_block):
            first, second, third = [
                final[f][s_slots[f, 0, b * per_block + j]] for f in range(3)
            ]
            keys += [first, second[0:16]]
            values += [second[16:48], third]
        keys = jnp.concatenate(keys, axis=0)
        values = jnp.concatenate([jnp.concatenate(values, axis=0), ones], axis=1)
        q = v_q[b].reshape(heads_rows, HD)
        scores = lax.dot_general(q, keys, (((1,), (1,)), ((), ())), preferred_element_type=F32)
        top = jnp.max(scores, axis=-1, keepdims=True)
        weight = jnp.exp(scores - top).astype(BF)
        value = jnp.dot(weight, values, preferred_element_type=F32)
        value = (value[:, :HD] / value[:, HD:]).astype(BF)
        at = pl.ds(b * PLEN, PLEN)
        for h in range(n_heads):
            v_att[at, pl.ds(h * HD, HD)] = value[h * PLEN : (h + 1) * PLEN]

    def att_copy(i):
        return pltpu.make_async_remote_copy(
            src_ref=v_att.at[pl.ds(i * chunk, chunk)],
            dst_ref=v_attp.at[pl.ds(i * chunk, chunk)],
            send_sem=att_ss.at[i],
            recv_sem=att_rs.at[i],
            device_id=(st, other),
            device_id_type=MESH,
        )

    n_chunks = rows_tok // chunk

    def attend_chunk(i, carry):
        per = n_blocks // n_chunks
        for k in range(per):
            attend(i * per + k)
        att_copy(i).start()
        return carry

    lax.fori_loop(0, n_chunks, attend_chunk, 0)

    mine = v_att.shape[1]

    def out_copy(i):
        at = pl.ds(i * chunk, chunk)
        return pltpu.make_async_copy(v_out.at[at], out.at[at], out_sem.at[i])

    def project(i, carry):
        at = pl.ds(pl.multiple_of(i * chunk, chunk), chunk)
        att_copy(i).wait_recv()
        cross = jnp.dot(
            v_att[at, :], v_wout[pl.ds(pl.multiple_of(tp * mine, mine), mine), :], preferred_element_type=F32
        )
        cross = cross + jnp.dot(
            v_attp[at, :],
            v_wout[pl.ds(pl.multiple_of(other * mine, mine), mine), :],
            preferred_element_type=F32,
        )
        v_out[at, :] = (v_conv[at, :] + jax.nn.sigmoid(gate_logit[...]) * cross).astype(BF)
        out_copy(i).start()
        return carry

    lax.fori_loop(0, n_chunks, project, 0)

    for i in range(n_chunks):
        out_copy(i).wait()
        att_copy(i).wait_send()
    for f in range(3):
        for o in OFFS:
            ask_first(f, o).wait_send()
            ask_second(f, o).wait_send()
    tok_remote.wait_send()
    for f in range(3):
        for o in OFFS:
            for p in range(4):
                a_copy(f, o, p).wait_send()
        for group in range(2):
            for ob in OFFS:
                for cp in b_copies(f, group, ob):
                    cp.wait_send()
            for oc in OFFS:
                for ob in range(RING):
                    c_copy(f, group, oc, ob).wait_send()


def on_device(
    tokens,
    norm_gain,
    branch_outer,
    branch_gate,
    branch_input,
    conv_taps,
    query_weight,
    query_gain,
    head_scale,
    store,
    store_gain,
    key_weight,
    value_weight,
    key_gain,
    out_weight,
    gate_logit,
    passage_ids,
):
    n_pass, plen, width = store.shape
    n_tok, half = tokens.shape
    heads = head_scale.shape[0]
    n_st = lax.axis_size("st")
    blocks = passage_ids.shape[0]

    vmem = pl.BlockSpec(memory_space=pltpu.VMEM)
    smem = pl.BlockSpec(memory_space=pltpu.SMEM)
    hbm = pl.BlockSpec(memory_space=pl.ANY)
    dma = pltpu.SemaphoreType.DMA
    scratch = [
        pltpu.VMEM((n_pass * plen, width), BF),
        pltpu.VMEM((width, 2 * HD), BF),
        pltpu.VMEM((256, width), BF),
        pltpu.VMEM((2, n_tok, half), BF),
        pltpu.VMEM((n_tok, width), BF),
        pltpu.VMEM(branch_outer.shape, BF),
        pltpu.VMEM(branch_gate.shape, BF),
        pltpu.VMEM(branch_input.shape, BF),
        pltpu.VMEM(query_weight.shape, BF),
        pltpu.VMEM(out_weight.shape, BF),
        pltpu.VMEM((blocks, heads, plen, HD), BF),
        pltpu.VMEM((n_tok, half), F32),
        pltpu.VMEM((n_tok, heads * HD), BF),
        pltpu.VMEM((n_tok, heads * HD), BF),
        pltpu.VMEM((n_tok, half), BF),
        pltpu.VMEM((3, RING, RING, 1, n_st * CAP), jnp.int32),
        pltpu.SMEM((3, RING, RING, 1, n_st * CAP), jnp.int32),
        pltpu.VMEM((n_st * CAP, n_st * CAP), jnp.int32),
        pltpu.VMEM((3, 1, n_st * CAP), jnp.int32),
        pltpu.SMEM((3, 1, n_st * CAP), jnp.int32),
    ]
    for f in range(3):
        scratch += [pltpu.VMEM((n_pass, ROWS[f], HD), BF)] * RING
    for f in range(3):
        scratch += [pltpu.VMEM((RING, RING, len(g) * CAP, ROWS[f], HD), BF) for g in GROUP]
    for f in range(3):
        scratch += [pltpu.VMEM((3, 3, len(g) * CAP, ROWS[f], HD), BF) for g in GROUP]
    for f in range(3):
        scratch += [pltpu.VMEM((n_st * CAP, ROWS[f], HD), BF)]
    scratch += [
        dma((10,)),
        dma((4,)),
        dma((4,)),
        dma((3, 6)),
        dma((3, 6)),
        dma,
        dma,
        dma((9, 4)),
        dma((9, 4)),
        dma((18, 2)),
        dma((18, 2)),
        dma((72,)),
        dma((72,)),
        dma((4,)),
        dma((4,)),
    ]
    return pl.pallas_call(
        kernel,
        out_shape=jax.ShapeDtypeStruct((n_tok, half), BF),
        in_specs=[
            smem,
            hbm,
            vmem,
            hbm,
            hbm,
            hbm,
            vmem,
            hbm,
            vmem,
            smem,
            hbm,
            vmem,
            hbm,
            hbm,
            vmem,
            hbm,
            vmem,
        ],
        out_specs=hbm,
        scratch_shapes=scratch,
        compiler_params=pltpu.CompilerParams(
            collective_id=0, has_side_effects=True, vmem_limit_bytes=56 * 1024 * 1024
        ),
    )(
        passage_ids.T,
        tokens,
        norm_gain.reshape(1, -1),
        branch_outer,
        branch_gate,
        branch_input,
        conv_taps,
        query_weight,
        query_gain.reshape(1, -1),
        head_scale,
        store.reshape(n_pass * plen, width),
        store_gain.reshape(1, -1),
        key_weight,
        value_weight,
        key_gain.reshape(1, -1),
        out_weight,
        gate_logit.reshape(1, -1),
    )


def solution(mesh):
    return jax.shard_map(
        on_device,
        mesh=mesh,
        in_specs=(
            P("st", "tp"),
            P(),
            P(None, "tp"),
            P(None, "tp"),
            P(None, "tp"),
            P(None, "tp"),
            P(None, "tp"),
            P(),
            P("tp"),
            P("st", None, None),
            P(),
            P(None, "tp"),
            P(None, "tp"),
            P(),
            P(None, "tp"),
            P("tp"),
            P("st", None),
        ),
        out_specs=P("st", "tp"),
        check_vma=False,
    )
```

```python
import math

import jax
import jax.numpy as jnp
from jax import lax
from jax.experimental import pallas as pl
from jax.experimental.pallas import tpu as pltpu
from jax.sharding import PartitionSpec as P

MESH = pl.DeviceIdType.MESH
EPS = 1e-06
SEQ = 128
RING = 4
CAP = 2
HD = 128
PLEN = 64
BF = jnp.bfloat16
F32 = jnp.float32

ORDERS = (("z", "y", "x"), ("y", "x", "z"), ("x", "z", "y"))
ROWS = (40, 40, 48)
STRIDE = {"z": RING * RING, "y": RING, "x": 1}
GROUP = ((0,), (1, 3), (2,))
START = (0, RING * RING * CAP, RING * RING * CAP * 3)
OFFS = (1, 3, 2)


def coordinates(st):
    return {"z": st // 16, "y": lax.rem(st // 4, 4), "x": lax.rem(st, 4)}


def shifted(st, moves):
    at = coordinates(st)
    out = 0
    for axis in ("z", "y", "x"):
        out = out + lax.rem(at[axis] + (moves.get(axis, 0) % RING), RING) * STRIDE[axis]
    return out


def position(group, oc, ob):
    return START[group] + (oc * RING + ob) * len(GROUP[group]) * CAP


def kernel(
    ids,
    tokens,
    norm_gain,
    w_outer,
    w_gate,
    w_input,
    taps,
    w_query,
    query_gain,
    head_scale,
    store,
    store_gain,
    w_key,
    w_value,
    key_gain,
    w_out,
    gate_logit,
    out,
    v_store,
    v_wkv,
    v_mem,
    v_x,
    v_n,
    v_wo,
    v_wg,
    v_wi,
    v_wq,
    v_wout,
    v_q,
    v_conv,
    v_att,
    v_attp,
    v_out,
    v_ask,
    s_ask,
    v_put,
    v_slots,
    s_slots,
    *rest,
):
    table = [rest[f * 4 : f * 4 + 4] for f in range(3)]
    rest = rest[12:]
    packed = [rest[f * 3 : f * 3 + 3] for f in range(3)]
    rest = rest[9:]
    relay = [rest[f * 3 : f * 3 + 3] for f in range(3)]
    rest = rest[9:]
    final = rest[:3]
    (
        local_sem,
        store_sem,
        out_sem,
        ask_ss,
        ask_rs,
        tok_ss,
        tok_rs,
        a_ss,
        a_rs,
        b_ss,
        b_rs,
        c_ss,
        c_rs,
        att_ss,
        att_rs,
    ) = rest[3:]

    st = lax.axis_index("st")
    tp = lax.axis_index("tp")
    other = 1 - tp
    rows_tok = tokens.shape[0]
    half = tokens.shape[1]
    width = 2 * half
    n_pass = store.shape[0] // PLEN

    store_copies = []
    wk = pltpu.make_async_copy(w_key, v_wkv.at[:, pl.ds(0, HD)], local_sem.at[0])
    wv = pltpu.make_async_copy(w_value, v_wkv.at[:, pl.ds(HD, HD)], local_sem.at[1])
    chunk = 256
    for p in range(4):
        store_copies.append(
            pltpu.make_async_copy(
                store.at[pl.ds(p * chunk, chunk)], v_store.at[pl.ds(p * chunk, chunk)], store_sem.at[p]
            )
        )
    store_copies[0].start()
    wk.start()
    wv.start()
    for p in range(1, 4):
        store_copies[p].start()
    tok_local = pltpu.make_async_copy(tokens, v_x.at[tp], local_sem.at[2])
    tok_local.start()
    weights = []
    for i, (src, dst) in enumerate(
        ((w_query, v_wq), (w_outer, v_wo), (w_gate, v_wg), (w_input, v_wi), (w_out, v_wout))
    ):
        cp = pltpu.make_async_copy(src, dst, local_sem.at[3 + i])
        cp.start()
        weights.append(cp)

    barrier = pltpu.get_barrier_semaphore()
    for axis in STRIDE:
        for o in OFFS:
            pl.semaphore_signal(barrier, inc=1, device_id=(shifted(st, {axis: o}), tp), device_id_type=MESH)
    pl.semaphore_signal(barrier, inc=1, device_id=(st, other), device_id_type=MESH)

    lanes = v_put.shape[1]
    lane = lax.broadcasted_iota(jnp.int32, (1, lanes), 1)
    lane_owner = lane // CAP
    lane_rank = lax.rem(lane, CAP)
    per_block, n_blocks = ids.shape
    v_put[...] = jnp.zeros_like(v_put)

    def request(j, carry):
        wanted, count = carry
        for p in range(per_block):
            number = ids[p, j]
            owner = lax.div(number, n_pass)
            match = lane_owner == owner
            put = match & (count == lane_rank)
            wanted = jnp.where(put, number - owner * n_pass, wanted)
            count = count + match.astype(jnp.int32)
            v_put[pl.ds(j * per_block + p, 1), :] = put.astype(jnp.int32)
        return wanted, count

    zero = jnp.zeros((1, lanes), jnp.int32)
    wanted, _ = lax.fori_loop(0, n_blocks, request, (zero, zero), unroll=4)
    for f in range(3):
        v_ask[f, 0, 0] = wanted
    me = coordinates(st)
    them = {
        "z": lane_owner // (RING * RING),
        "y": lax.rem(lane_owner // RING, RING),
        "x": lax.rem(lane_owner, RING),
    }
    for f in range(3):
        oa, ob, oc = [lax.rem(me[axis] - them[axis] + RING, RING) for axis in ORDERS[f]]
        spot = oc * RING + ob
        where = jnp.zeros_like(lane)
        for group, members in enumerate(GROUP):
            for j, o in enumerate(members):
                first = START[group] + spot * (len(members) * CAP) + j * CAP
                where = jnp.where(oa == o, first + lane_rank, where)
        spots = v_put[...] * where
        v_slots[f] = jnp.sum(spots.T, axis=0, keepdims=True)

    def ask_first(f, oc):
        return pltpu.make_async_remote_copy(
            src_ref=v_ask.at[f, 0, 0],
            dst_ref=v_ask.at[f, 0, oc],
            send_sem=ask_ss.at[f, oc - 1],
            recv_sem=ask_rs.at[f, oc - 1],
            device_id=(shifted(st, {ORDERS[f][2]: -oc}), tp),
            device_id_type=MESH,
        )

    def ask_second(f, ob):
        return pltpu.make_async_remote_copy(
            src_ref=v_ask.at[f, 0],
            dst_ref=v_ask.at[f, ob],
            send_sem=ask_ss.at[f, 2 + ob],
            recv_sem=ask_rs.at[f, 2 + ob],
            device_id=(shifted(st, {ORDERS[f][1]: -ob}), tp),
            device_id_type=MESH,
        )

    tok_remote = pltpu.make_async_remote_copy(
        src_ref=tokens,
        dst_ref=v_x.at[tp],
        send_sem=tok_ss,
        recv_sem=tok_rs,
        device_id=(st, other),
        device_id_type=MESH,
    )

    def a_copy(f, o, p):
        ahead = o == 1 or (o == 2 and p < 2)
        src = table[f][0] if o != 2 else table[f][1 if ahead else 3]
        return a_step(f, o, p, src, 1 if ahead else 3)

    def a_step(f, o, p, src, move):
        return pltpu.make_async_remote_copy(
            src_ref=src.at[pl.ds(p * 4, 4)],
            dst_ref=table[f][o].at[pl.ds(p * 4, 4)],
            send_sem=a_ss.at[f * 3 + o - 1, p],
            recv_sem=a_rs.at[f * 3 + o - 1, p],
            device_id=(shifted(st, {ORDERS[f][0]: move}), tp),
            device_id_type=MESH,
        )

    wk.wait()
    wv.wait()
    sub = 32

    def kv_chunk(p, carry):
        base = p * chunk
        pltpu.make_async_copy(
            store.at[pl.ds(base, chunk)], v_store.at[pl.ds(base, chunk)], store_sem.at[p]
        ).wait()

        def norm_sub(i, c):
            x = v_store[pl.ds(base + i * sub, sub), :].astype(F32)
            r = lax.rsqrt(jnp.mean(x * x, axis=-1, keepdims=True) + EPS)
            v_mem[pl.ds(i * sub, sub), :] = (x * r * store_gain[...]).astype(BF)
            return c

        lax.fori_loop(0, chunk // sub, norm_sub, 0, unroll=2)
        kv = jnp.dot(v_mem[...], v_wkv[...], preferred_element_type=F32)
        k = kv[:, :HD]
        k = k * lax.rsqrt(jnp.mean(k * k, axis=-1, keepdims=True) + EPS) * key_gain[...]
        k = k.astype(BF).reshape(4, PLEN, HD)
        v = kv[:, HD:].astype(BF).reshape(4, PLEN, HD)
        at = pl.ds(p * 4, 4)
        table[0][0][at, 0:32, :] = k[:, 0:32]
        table[0][0][at, 32:40, :] = v[:, 48:56]
        table[1][0][at, 0:32, :] = k[:, 32:64]
        table[1][0][at, 32:40, :] = v[:, 56:64]
        table[2][0][at, :, :] = v[:, 0:48]

        @pl.when(p == 0)
        def _():
            pl.semaphore_wait(barrier, 3 * len(OFFS) + 1)
            for f in range(3):
                for oc in OFFS:
                    ask_first(f, oc).start()

        for f in range(3):
            for o in (1, 3):
                a_step(f, o, p, table[f][0], o).start()

        @pl.when(p == 0)
        def _():
            tok_remote.start()

        @pl.when(p == 2)
        def _():
            for f in range(3):
                for oc in OFFS:
                    ask_first(f, oc).wait_recv()
            for f in range(3):
                for ob in OFFS:
                    ask_second(f, ob).start()

        return carry

    lax.fori_loop(0, 4, kv_chunk, 0)

    def pack(group):
        n = len(GROUP[group]) * CAP
        for f in range(3):
            owners = [shifted(st, {ORDERS[f][0]: -o}) for o in GROUP[group]]

            def one(t, carry, f=f, owners=owners):
                ob = t // RING
                oc = lax.rem(t, RING)
                for j, o in enumerate(GROUP[group]):
                    for r in range(CAP):
                        at = s_ask[f, ob, oc, 0, owners[j] * CAP + r]
                        packed[f][group][ob, oc, j * CAP + r] = table[f][o][at]
                return carry

            lax.fori_loop(0, RING * RING, one, 0, unroll=2)
            final[f][pl.ds(position(group, 0, 0), n)] = packed[f][group][0, 0]

    def b_copies(f, group, ob):
        n = len(GROUP[group]) * CAP
        to = (shifted(st, {ORDERS[f][1]: ob}), tp)
        i = (f * 3 + group) * 3 + ob - 1
        return (
            pltpu.make_async_remote_copy(
                src_ref=packed[f][group].at[ob, pl.ds(1, 3)],
                dst_ref=relay[f][group].at[ob - 1],
                send_sem=b_ss.at[i, 0],
                recv_sem=b_rs.at[i, 0],
                device_id=to,
                device_id_type=MESH,
            ),
            pltpu.make_async_remote_copy(
                src_ref=packed[f][group].at[ob, 0],
                dst_ref=final[f].at[pl.ds(position(group, 0, ob), n)],
                send_sem=b_ss.at[i, 1],
                recv_sem=b_rs.at[i, 1],
                device_id=to,
                device_id_type=MESH,
            ),
        )

    def c_copy(f, group, oc, ob):
        n = len(GROUP[group]) * CAP
        i = ((f * 3 + group) * 3 + oc - 1) * 4 + ob
        src = packed[f][group].at[0, oc] if ob == 0 else relay[f][group].at[ob - 1, oc - 1]
        return pltpu.make_async_remote_copy(
            src_ref=src,
            dst_ref=final[f].at[pl.ds(position(group, oc, ob), n)],
            send_sem=c_ss.at[i],
            recv_sem=c_rs.at[i],
            device_id=(shifted(st, {ORDERS[f][2]: oc}), tp),
            device_id_type=MESH,
        )

    def send_packed(group):
        for f in range(3):
            for ob in OFFS:
                b_copies(f, group, ob)[0].start()
        for f in range(3):
            for ob in OFFS:
                b_copies(f, group, ob)[1].start()
        for f in range(3):
            for oc in OFFS:
                c_copy(f, group, oc, 0).start()

    def forward(group, ob):
        for f in range(3):
            b_copies(f, group, ob)[0].wait_recv()
            for oc in OFFS:
                c_copy(f, group, oc, ob).start()

    tok_local.wait()

    def norm_tok(i, c):
        at = pl.ds(i * sub, sub)
        x0 = v_x[0, at, :].astype(F32)
        x1 = v_x[1, at, :].astype(F32)
        total = jnp.sum(x0 * x0, axis=-1, keepdims=True) + jnp.sum(x1 * x1, axis=-1, keepdims=True)
        r = lax.rsqrt(total * (1.0 / width) + EPS)
        v_n[at, pl.ds(0, half)] = (x0 * r * norm_gain[:, 0:half]).astype(BF)
        v_n[at, pl.ds(half, half)] = (x1 * r * norm_gain[:, half:width]).astype(BF)
        return c

    tok_remote.wait_recv()
    n_sub = rows_tok // sub
    quarter = n_sub // 4
    lax.fori_loop(0, quarter, norm_tok, 0, unroll=2)

    def onward(p):
        for f in range(3):
            a_copy(f, 1 if p < 2 else 3, p).wait_recv()
            a_copy(f, 2, p).start()

    onward(0)
    onward(1)
    lax.fori_loop(quarter, 2 * quarter, norm_tok, 0, unroll=2)
    onward(2)
    onward(3)
    for f in range(3):
        for ob in OFFS:
            ask_second(f, ob).wait_recv()
    ask_local = pltpu.make_async_copy(v_ask, s_ask, local_sem.at[8])
    ask_local.start()
    slots_local = pltpu.make_async_copy(v_slots, s_slots, local_sem.at[9])
    slots_local.start()
    ask_local.wait()
    slots_local.wait()
    pack(0)
    send_packed(0)
    for f in range(3):
        for p in range(4):
            a_copy(f, 3 if p < 2 else 1, p).wait_recv()
    pack(1)
    send_packed(1)
    lax.fori_loop(2 * quarter, n_sub, norm_tok, 0, unroll=2)
    for f in range(3):
        for p in range(4):
            a_copy(f, 2, p).wait_recv()
    pack(2)
    send_packed(2)

    weights[0].wait()
    n_heads = v_q.shape[1]

    def query_chunk(i, c):
        raw = jnp.dot(v_n[pl.ds(i * chunk, chunk), :], v_wq[...], preferred_element_type=F32)
        for h in range(n_heads):
            q = raw[:, h * HD : (h + 1) * HD]
            q = q * lax.rsqrt(jnp.mean(q * q, axis=-1, keepdims=True) + EPS) * query_gain[...]
            q = (q * (head_scale[h] / math.sqrt(HD))).astype(BF).reshape(chunk // PLEN, PLEN, HD)
            v_q[pl.ds(i * (chunk // PLEN), chunk // PLEN), h] = q
        return c

    lax.fori_loop(0, rows_tok // chunk, query_chunk, 0)

    for cp in weights[1:4]:
        cp.wait()
    tall, wide = 512, 256
    cols = v_wo.shape[1] // wide

    def branch(s, carry):
        rows = pl.ds(pl.multiple_of((s // cols) * tall, tall), tall)
        at = pl.ds(pl.multiple_of(lax.rem(s, cols) * wide, wide), wide)
        n = v_n[rows, :]
        gate = jnp.dot(n, v_wg[:, at], preferred_element_type=F32)
        z = gate * jnp.dot(n, v_wi[:, at], preferred_element_type=F32)
        row = lax.rem(lax.broadcasted_iota(jnp.int32, (tall, wide), 0), SEQ)
        one = jnp.where(row >= 1, pltpu.roll(z, 1, 0), 0.0)
        two = jnp.where(row >= 2, pltpu.roll(z, 2, 0), 0.0)
        t = taps[:, at]
        conv = two * t[0:1] + one * t[1:2] + z * t[2:3]
        v_conv[rows, at] = conv
        v_conv[rows, at] = (
            jnp.dot(n, v_wo[:, at], preferred_element_type=F32) * v_conv[rows, at]
        )

        @pl.when(s == 0)
        def _():
            for ob in OFFS:
                forward(0, ob)

        @pl.when(s == 1)
        def _():
            forward(1, 1)
            forward(1, 3)

        @pl.when(s == 2)
        def _():
            forward(1, 2)

        @pl.when(s == 4)
        def _():
            for ob in OFFS:
                forward(2, ob)

        return carry

    lax.fori_loop(0, (rows_tok // tall) * cols, branch, 0)

    weights[4].wait()
    for f in range(3):
        for group in range(len(GROUP)):
            for ob in OFFS:
                b_copies(f, group, ob)[1].wait_recv()
            for oc in OFFS:
                for ob in range(RING):
                    c_copy(f, group, oc, ob).wait_recv()

    heads_rows = n_heads * PLEN
    ones = jnp.ones((per_block * PLEN, HD), BF)

    def attend(b):
        keys, values = [], []
        for j in range(per_block):
            first, second, third = [
                final[f][s_slots[f, 0, b * per_block + j]] for f in range(3)
            ]
            keys += [first[0:32], second[0:32]]
            values += [third, first[32:40], second[32:40]]
        keys = jnp.concatenate(keys, axis=0)
        values = jnp.concatenate([jnp.concatenate(values, axis=0), ones], axis=1)
        q = v_q[b].reshape(heads_rows, HD)
        scores = lax.dot_general(q, keys, (((1,), (1,)), ((), ())), preferred_element_type=F32)
        top = jnp.max(scores, axis=-1, keepdims=True)
        weight = jnp.exp(scores - top).astype(BF)
        value = jnp.dot(weight, values, preferred_element_type=F32)
        value = (value[:, :HD] / value[:, HD:]).astype(BF)
        at = pl.ds(b * PLEN, PLEN)
        for h in range(n_heads):
            v_att[at, pl.ds(h * HD, HD)] = value[h * PLEN : (h + 1) * PLEN]

    def att_copy(i):
        return pltpu.make_async_remote_copy(
            src_ref=v_att.at[pl.ds(i * chunk, chunk)],
            dst_ref=v_attp.at[pl.ds(i * chunk, chunk)],
            send_sem=att_ss.at[i],
            recv_sem=att_rs.at[i],
            device_id=(st, other),
            device_id_type=MESH,
        )

    n_chunks = rows_tok // chunk

    def attend_chunk(i, carry):
        per = n_blocks // n_chunks
        for k in range(per):
            attend(i * per + k)
        att_copy(i).start()
        return carry

    lax.fori_loop(0, n_chunks, attend_chunk, 0)

    mine = v_att.shape[1]

    def out_copy(i):
        at = pl.ds(i * chunk, chunk)
        return pltpu.make_async_copy(v_out.at[at], out.at[at], out_sem.at[i])

    def project(i, carry):
        at = pl.ds(pl.multiple_of(i * chunk, chunk), chunk)
        att_copy(i).wait_recv()
        cross = jnp.dot(
            v_att[at, :], v_wout[pl.ds(pl.multiple_of(tp * mine, mine), mine), :], preferred_element_type=F32
        )
        cross = cross + jnp.dot(
            v_attp[at, :],
            v_wout[pl.ds(pl.multiple_of(other * mine, mine), mine), :],
            preferred_element_type=F32,
        )
        v_out[at, :] = (v_conv[at, :] + jax.nn.sigmoid(gate_logit[...]) * cross).astype(BF)
        out_copy(i).start()
        return carry

    lax.fori_loop(0, n_chunks, project, 0)

    for i in range(n_chunks):
        out_copy(i).wait()
        att_copy(i).wait_send()
    for f in range(3):
        for o in OFFS:
            ask_first(f, o).wait_send()
            ask_second(f, o).wait_send()
    tok_remote.wait_send()
    for f in range(3):
        for o in OFFS:
            for p in range(4):
                a_copy(f, o, p).wait_send()
        for group in range(len(GROUP)):
            for ob in OFFS:
                for cp in b_copies(f, group, ob):
                    cp.wait_send()
            for oc in OFFS:
                for ob in range(RING):
                    c_copy(f, group, oc, ob).wait_send()


def on_device(
    tokens,
    norm_gain,
    branch_outer,
    branch_gate,
    branch_input,
    conv_taps,
    query_weight,
    query_gain,
    head_scale,
    store,
    store_gain,
    key_weight,
    value_weight,
    key_gain,
    out_weight,
    gate_logit,
    passage_ids,
):
    n_pass, plen, width = store.shape
    n_tok, half = tokens.shape
    heads = head_scale.shape[0]
    n_st = lax.axis_size("st")
    blocks = passage_ids.shape[0]

    vmem = pl.BlockSpec(memory_space=pltpu.VMEM)
    smem = pl.BlockSpec(memory_space=pltpu.SMEM)
    hbm = pl.BlockSpec(memory_space=pl.ANY)
    dma = pltpu.SemaphoreType.DMA
    scratch = [
        pltpu.VMEM((n_pass * plen, width), BF),
        pltpu.VMEM((width, 2 * HD), BF),
        pltpu.VMEM((256, width), BF),
        pltpu.VMEM((2, n_tok, half), BF),
        pltpu.VMEM((n_tok, width), BF),
        pltpu.VMEM(branch_outer.shape, BF),
        pltpu.VMEM(branch_gate.shape, BF),
        pltpu.VMEM(branch_input.shape, BF),
        pltpu.VMEM(query_weight.shape, BF),
        pltpu.VMEM(out_weight.shape, BF),
        pltpu.VMEM((blocks, heads, plen, HD), BF),
        pltpu.VMEM((n_tok, half), F32),
        pltpu.VMEM((n_tok, heads * HD), BF),
        pltpu.VMEM((n_tok, heads * HD), BF),
        pltpu.VMEM((n_tok, half), BF),
        pltpu.VMEM((3, RING, RING, 1, n_st * CAP), jnp.int32),
        pltpu.SMEM((3, RING, RING, 1, n_st * CAP), jnp.int32),
        pltpu.VMEM((n_st * CAP, n_st * CAP), jnp.int32),
        pltpu.VMEM((3, 1, n_st * CAP), jnp.int32),
        pltpu.SMEM((3, 1, n_st * CAP), jnp.int32),
    ]
    for f in range(3):
        scratch += [pltpu.VMEM((n_pass, ROWS[f], HD), BF)] * RING
    for f in range(3):
        scratch += [pltpu.VMEM((RING, RING, len(g) * CAP, ROWS[f], HD), BF) for g in GROUP]
    for f in range(3):
        scratch += [pltpu.VMEM((3, 3, len(g) * CAP, ROWS[f], HD), BF) for g in GROUP]
    for f in range(3):
        scratch += [pltpu.VMEM((n_st * CAP, ROWS[f], HD), BF)]
    scratch += [
        dma((10,)),
        dma((4,)),
        dma((4,)),
        dma((3, 6)),
        dma((3, 6)),
        dma,
        dma,
        dma((9, 4)),
        dma((9, 4)),
        dma((27, 2)),
        dma((27, 2)),
        dma((108,)),
        dma((108,)),
        dma((4,)),
        dma((4,)),
    ]
    return pl.pallas_call(
        kernel,
        out_shape=jax.ShapeDtypeStruct((n_tok, half), BF),
        in_specs=[
            smem,
            hbm,
            vmem,
            hbm,
            hbm,
            hbm,
            vmem,
            hbm,
            vmem,
            smem,
            hbm,
            vmem,
            hbm,
            hbm,
            vmem,
            hbm,
            vmem,
        ],
        out_specs=hbm,
        scratch_shapes=scratch,
        compiler_params=pltpu.CompilerParams(
            collective_id=0, has_side_effects=True, vmem_limit_bytes=56 * 1024 * 1024
        ),
    )(
        passage_ids.T,
        tokens,
        norm_gain.reshape(1, -1),
        branch_outer,
        branch_gate,
        branch_input,
        conv_taps,
        query_weight,
        query_gain.reshape(1, -1),
        head_scale,
        store.reshape(n_pass * plen, width),
        store_gain.reshape(1, -1),
        key_weight,
        value_weight,
        key_gain.reshape(1, -1),
        out_weight,
        gate_logit.reshape(1, -1),
    )


def solution(mesh):
    return jax.shard_map(
        on_device,
        mesh=mesh,
        in_specs=(
            P("st", "tp"),
            P(),
            P(None, "tp"),
            P(None, "tp"),
            P(None, "tp"),
            P(None, "tp"),
            P(None, "tp"),
            P(),
            P("tp"),
            P("st", None, None),
            P(),
            P(None, "tp"),
            P(None, "tp"),
            P(),
            P(None, "tp"),
            P("tp"),
            P("st", None),
        ),
        out_specs=P("st", "tp"),
        check_vma=False,
    )
```

```python
import math

import jax
import jax.numpy as jnp
from jax import lax
from jax.experimental import pallas as pl
from jax.experimental.pallas import tpu as pltpu
from jax.sharding import PartitionSpec as P

MESH = pl.DeviceIdType.MESH
EPS = 1e-06
SEQ = 128
RING = 4
CAP = 2
HD = 128
PLEN = 64
BF = jnp.bfloat16
F32 = jnp.float32

ORDERS = (("z", "y", "x"), ("y", "x", "z"), ("x", "z", "y"))
ROWS = (40, 40, 48)
STRIDE = {"z": RING * RING, "y": RING, "x": 1}
GROUP = ((0,), (1, 3), (2,))
START = (0, RING * RING * CAP, RING * RING * CAP * 3)
OFFS = (1, 3, 2)
PLACE = {0: 0, 1: 1, 3: 2, 2: 3}
PARTS = ((0,), (1, 3), (2,))


def coordinates(st):
    return {"z": st // 16, "y": lax.rem(st // 4, 4), "x": lax.rem(st, 4)}


def shifted(st, moves):
    at = coordinates(st)
    out = 0
    for axis in ("z", "y", "x"):
        out = out + lax.rem(at[axis] + (moves.get(axis, 0) % RING), RING) * STRIDE[axis]
    return out


def position(group, oc, ob):
    return START[group] + (oc * RING + PLACE[ob]) * len(GROUP[group]) * CAP


def place(group, ob):
    return (PLACE[ob] - 1) * len(GROUP[group]) * CAP


def kernel(
    ids,
    tokens,
    norm_gain,
    w_outer,
    w_gate,
    w_input,
    taps,
    w_query,
    query_gain,
    head_scale,
    store,
    store_gain,
    w_key,
    w_value,
    key_gain,
    w_out,
    gate_logit,
    out,
    v_store,
    v_wkv,
    v_mem,
    v_x,
    v_n,
    v_wo,
    v_wg,
    v_wi,
    v_wq,
    v_wout,
    v_q,
    v_conv,
    v_att,
    v_attp,
    v_out,
    v_ask,
    s_near,
    s_ask,
    v_put,
    v_slots,
    s_slots,
    *rest,
):
    table = [rest[f * 4 : f * 4 + 4] for f in range(3)]
    rest = rest[12:]
    packed = [rest[f * 3 : f * 3 + 3] for f in range(3)]
    rest = rest[9:]
    relay = [rest[f * 3 : f * 3 + 3] for f in range(3)]
    rest = rest[9:]
    final = rest[:3]
    (
        local_sem,
        store_sem,
        out_sem,
        ask_ss,
        ask_rs,
        tok_ss,
        tok_rs,
        a_ss,
        a_rs,
        b_ss,
        b_rs,
        c_ss,
        c_rs,
        att_ss,
        att_rs,
    ) = rest[3:]

    st = lax.axis_index("st")
    tp = lax.axis_index("tp")
    other = 1 - tp
    rows_tok = tokens.shape[0]
    half = tokens.shape[1]
    width = 2 * half
    n_pass = store.shape[0] // PLEN

    store_copies = []
    wk = pltpu.make_async_copy(w_key, v_wkv.at[:, pl.ds(0, HD)], local_sem.at[0])
    wv = pltpu.make_async_copy(w_value, v_wkv.at[:, pl.ds(HD, HD)], local_sem.at[1])
    chunk = 256
    for p in range(4):
        store_copies.append(
            pltpu.make_async_copy(
                store.at[pl.ds(p * chunk, chunk)], v_store.at[pl.ds(p * chunk, chunk)], store_sem.at[p]
            )
        )
    store_copies[0].start()
    wk.start()
    wv.start()
    for p in range(1, 4):
        store_copies[p].start()
    tok_local = pltpu.make_async_copy(tokens, v_x.at[tp], local_sem.at[2])
    tok_local.start()
    weights = []
    for i, (src, dst) in enumerate(
        ((w_query, v_wq), (w_outer, v_wo), (w_gate, v_wg), (w_input, v_wi), (w_out, v_wout))
    ):
        cp = pltpu.make_async_copy(src, dst, local_sem.at[3 + i])
        cp.start()
        weights.append(cp)

    barrier = pltpu.get_barrier_semaphore()
    for axis in STRIDE:
        for o in OFFS:
            pl.semaphore_signal(barrier, inc=1, device_id=(shifted(st, {axis: o}), tp), device_id_type=MESH)
    pl.semaphore_signal(barrier, inc=1, device_id=(st, other), device_id_type=MESH)

    lanes = v_put.shape[1]
    lane = lax.broadcasted_iota(jnp.int32, (1, lanes), 1)
    lane_owner = lane // CAP
    lane_rank = lax.rem(lane, CAP)
    per_block, n_blocks = ids.shape
    v_put[...] = jnp.zeros_like(v_put)

    def request(j, carry):
        wanted, count = carry
        for p in range(per_block):
            number = ids[p, j]
            owner = lax.div(number, n_pass)
            match = lane_owner == owner
            put = match & (count == lane_rank)
            wanted = jnp.where(put, number - owner * n_pass, wanted)
            count = count + match.astype(jnp.int32)
            v_put[pl.ds(j * per_block + p, 1), :] = put.astype(jnp.int32)
        return wanted, count

    zero = jnp.zeros((1, lanes), jnp.int32)
    wanted, _ = lax.fori_loop(0, n_blocks, request, (zero, zero), unroll=4)
    for f in range(3):
        v_ask[f, 0, 0] = wanted
    me = coordinates(st)
    them = {
        "z": lane_owner // (RING * RING),
        "y": lax.rem(lane_owner // RING, RING),
        "x": lax.rem(lane_owner, RING),
    }
    for f in range(3):
        oa, ob, oc = [lax.rem(me[axis] - them[axis] + RING, RING) for axis in ORDERS[f]]
        spot = oc * RING + jnp.where(ob == 2, 3, jnp.where(ob == 3, 2, ob))
        where = jnp.zeros_like(lane)
        for group, members in enumerate(GROUP):
            for j, o in enumerate(members):
                first = START[group] + spot * (len(members) * CAP) + j * CAP
                where = jnp.where(oa == o, first + lane_rank, where)
        spots = v_put[...] * where
        v_slots[f] = jnp.sum(spots.T, axis=0, keepdims=True)

    def ask_first(f, oc):
        return pltpu.make_async_remote_copy(
            src_ref=v_ask.at[f, 0, 0],
            dst_ref=v_ask.at[f, 0, oc],
            send_sem=ask_ss.at[f, oc - 1],
            recv_sem=ask_rs.at[f, oc - 1],
            device_id=(shifted(st, {ORDERS[f][2]: -oc}), tp),
            device_id_type=MESH,
        )

    def ask_second(f, ob):
        return pltpu.make_async_remote_copy(
            src_ref=v_ask.at[f, 0],
            dst_ref=v_ask.at[f, ob],
            send_sem=ask_ss.at[f, 2 + ob],
            recv_sem=ask_rs.at[f, 2 + ob],
            device_id=(shifted(st, {ORDERS[f][1]: -ob}), tp),
            device_id_type=MESH,
        )

    tok_remote = pltpu.make_async_remote_copy(
        src_ref=tokens,
        dst_ref=v_x.at[tp],
        send_sem=tok_ss,
        recv_sem=tok_rs,
        device_id=(st, other),
        device_id_type=MESH,
    )

    def a_copy(f, o, p):
        ahead = o == 1 or (o == 2 and p < 2)
        src = table[f][0] if o != 2 else table[f][1 if ahead else 3]
        return a_step(f, o, p, src, 1 if ahead else 3)

    def a_step(f, o, p, src, move):
        return pltpu.make_async_remote_copy(
            src_ref=src.at[pl.ds(p * 4, 4)],
            dst_ref=table[f][o].at[pl.ds(p * 4, 4)],
            send_sem=a_ss.at[f * 3 + o - 1, p],
            recv_sem=a_rs.at[f * 3 + o - 1, p],
            device_id=(shifted(st, {ORDERS[f][0]: move}), tp),
            device_id_type=MESH,
        )

    wk.wait()
    wv.wait()
    sub = 32

    def kv_chunk(p, carry):
        base = p * chunk
        pltpu.make_async_copy(
            store.at[pl.ds(base, chunk)], v_store.at[pl.ds(base, chunk)], store_sem.at[p]
        ).wait()

        def norm_sub(i, c):
            x = v_store[pl.ds(base + i * sub, sub), :].astype(F32)
            r = lax.rsqrt(jnp.mean(x * x, axis=-1, keepdims=True) + EPS)
            v_mem[pl.ds(i * sub, sub), :] = (x * r * store_gain[...]).astype(BF)
            return c

        lax.fori_loop(0, chunk // sub, norm_sub, 0, unroll=2)
        kv = jnp.dot(v_mem[...], v_wkv[...], preferred_element_type=F32)
        k = kv[:, :HD]
        k = k * lax.rsqrt(jnp.mean(k * k, axis=-1, keepdims=True) + EPS) * key_gain[...]
        k = k.astype(BF).reshape(4, PLEN, HD)
        v = kv[:, HD:].astype(BF).reshape(4, PLEN, HD)
        at = pl.ds(p * 4, 4)
        table[0][0][at, 0:32, :] = k[:, 0:32]
        table[0][0][at, 32:40, :] = v[:, 48:56]
        table[1][0][at, 0:32, :] = k[:, 32:64]
        table[1][0][at, 32:40, :] = v[:, 56:64]
        table[2][0][at, :, :] = v[:, 0:48]

        @pl.when(p == 0)
        def _():
            pl.semaphore_wait(barrier, 3 * len(OFFS) + 1)
            for f in range(3):
                for oc in OFFS:
                    ask_first(f, oc).start()

        @pl.when(p == 3)
        def _():
            for f in range(3):
                for oc in OFFS:
                    ask_first(f, oc).wait_recv()
            for f in range(3):
                for ob in OFFS:
                    ask_second(f, ob).start()

        for f in range(3):
            for o in (1, 3):
                a_step(f, o, p, table[f][0], o).start()

        @pl.when(p == 0)
        def _():
            tok_remote.start()

        return carry

    lax.fori_loop(0, 4, kv_chunk, 0)

    def pack(group, near):
        n = len(GROUP[group]) * CAP
        for f in range(3):
            owners = [shifted(st, {ORDERS[f][0]: -o}) for o in GROUP[group]]

            def one(t, carry, f=f, owners=owners):
                ob = 0 if near else 1 + t // RING
                oc = lax.rem(t, RING)
                for j, o in enumerate(GROUP[group]):
                    for r in range(CAP):
                        lane_at = owners[j] * CAP + r
                        at = s_near[f, oc, 0, lane_at] if near else s_ask[f, ob, oc, 0, lane_at]
                        packed[f][group][ob, oc, j * CAP + r] = table[f][o][at]
                return carry

            lax.fori_loop(0, RING * (1 if near else RING - 1), one, 0, unroll=2)
            if near:
                final[f][pl.ds(position(group, 0, 0), n)] = packed[f][group][0, 0]

    def b_copy(f, group, ob):
        i = (f * 3 + group) * 3 + ob - 1
        return pltpu.make_async_remote_copy(
            src_ref=packed[f][group].at[ob],
            dst_ref=relay[f][group].at[:, pl.ds(place(group, ob), len(GROUP[group]) * CAP)],
            send_sem=b_ss.at[i],
            recv_sem=b_rs.at[i],
            device_id=(shifted(st, {ORDERS[f][1]: ob}), tp),
            device_id_type=MESH,
        )

    def c_copy(f, group, oc, part):
        obs = PARTS[part]
        n = len(GROUP[group]) * CAP * len(obs)
        i = ((f * 3 + group) * 3 + oc - 1) * 3 + part
        if part == 0:
            src = packed[f][group].at[0, oc]
        else:
            src = relay[f][group].at[oc, pl.ds(place(group, obs[0]), n)]
        return pltpu.make_async_remote_copy(
            src_ref=src,
            dst_ref=final[f].at[pl.ds(position(group, oc, obs[0]), n)],
            send_sem=c_ss.at[i],
            recv_sem=c_rs.at[i],
            device_id=(shifted(st, {ORDERS[f][2]: oc}), tp),
            device_id_type=MESH,
        )

    def send_packed(group):
        for f in range(3):
            for ob in OFFS:
                b_copy(f, group, ob).start()

    def send_near(group):
        for f in range(3):
            for oc in OFFS:
                c_copy(f, group, oc, 0).start()

    def forward(group, part):
        n = len(GROUP[group]) * CAP
        for f in range(3):
            for ob in PARTS[part]:
                b_copy(f, group, ob).wait_recv()
            for oc in OFFS:
                c_copy(f, group, oc, part).start()
            for ob in PARTS[part]:
                final[f][pl.ds(position(group, 0, ob), n)] = relay[f][group][0, pl.ds(place(group, ob), n)]

    tok_local.wait()

    def norm_tok(i, c):
        at = pl.ds(i * sub, sub)
        x0 = v_x[0, at, :].astype(F32)
        x1 = v_x[1, at, :].astype(F32)
        total = jnp.sum(x0 * x0, axis=-1, keepdims=True) + jnp.sum(x1 * x1, axis=-1, keepdims=True)
        r = lax.rsqrt(total * (1.0 / width) + EPS)
        v_n[at, pl.ds(0, half)] = (x0 * r * norm_gain[:, 0:half]).astype(BF)
        v_n[at, pl.ds(half, half)] = (x1 * r * norm_gain[:, half:width]).astype(BF)
        return c

    near_local = pltpu.make_async_copy(v_ask.at[:, 0], s_near, local_sem.at[8])
    near_local.start()
    slots_local = pltpu.make_async_copy(v_slots, s_slots, local_sem.at[9])
    slots_local.start()
    tok_remote.wait_recv()
    n_sub = rows_tok // sub
    quarter = n_sub // 4
    lax.fori_loop(0, quarter, norm_tok, 0, unroll=2)
    near_local.wait()
    slots_local.wait()
    pack(0, True)
    send_near(0)

    def onward(p):
        for f in range(3):
            a_copy(f, 1 if p < 2 else 3, p).wait_recv()
            a_copy(f, 2, p).start()

    onward(0)
    onward(1)
    lax.fori_loop(quarter, 2 * quarter, norm_tok, 0, unroll=2)
    onward(2)
    onward(3)
    for f in range(3):
        for p in range(4):
            a_copy(f, 3 if p < 2 else 1, p).wait_recv()
    pack(1, True)
    send_near(1)
    for f in range(3):
        for ob in OFFS:
            ask_second(f, ob).wait_recv()
    ask_local = pltpu.make_async_copy(v_ask, s_ask, local_sem.at[10])
    ask_local.start()
    ask_local.wait()
    for group in range(2):
        pack(group, False)
        send_packed(group)
    lax.fori_loop(2 * quarter, n_sub, norm_tok, 0, unroll=2)
    for f in range(3):
        for p in range(4):
            a_copy(f, 2, p).wait_recv()
    pack(2, False)
    send_packed(2)
    pack(2, True)
    send_near(2)

    weights[0].wait()
    n_heads = v_q.shape[1]

    def query_chunk(i, c):
        raw = jnp.dot(v_n[pl.ds(i * chunk, chunk), :], v_wq[...], preferred_element_type=F32)
        for h in range(n_heads):
            q = raw[:, h * HD : (h + 1) * HD]
            q = q * lax.rsqrt(jnp.mean(q * q, axis=-1, keepdims=True) + EPS) * query_gain[...]
            q = (q * (head_scale[h] / math.sqrt(HD))).astype(BF).reshape(chunk // PLEN, PLEN, HD)
            v_q[pl.ds(i * (chunk // PLEN), chunk // PLEN), h] = q
        return c

    lax.fori_loop(0, rows_tok // chunk, query_chunk, 0)

    for cp in weights[1:4]:
        cp.wait()
    tall, wide = 512, 256
    cols = v_wo.shape[1] // wide

    def branch(s, carry):
        rows = pl.ds(pl.multiple_of((s // cols) * tall, tall), tall)
        at = pl.ds(pl.multiple_of(lax.rem(s, cols) * wide, wide), wide)
        n = v_n[rows, :]
        gate = jnp.dot(n, v_wg[:, at], preferred_element_type=F32)
        z = gate * jnp.dot(n, v_wi[:, at], preferred_element_type=F32)
        row = lax.rem(lax.broadcasted_iota(jnp.int32, (tall, wide), 0), SEQ)
        one = jnp.where(row >= 1, pltpu.roll(z, 1, 0), 0.0)
        two = jnp.where(row >= 2, pltpu.roll(z, 2, 0), 0.0)
        t = taps[:, at]
        conv = two * t[0:1] + one * t[1:2] + z * t[2:3]
        v_conv[rows, at] = conv
        v_conv[rows, at] = (
            jnp.dot(n, v_wo[:, at], preferred_element_type=F32) * v_conv[rows, at]
        )

        @pl.when(s == 0)
        def _():
            forward(0, 1)
            forward(0, 2)

        @pl.when(s == 1)
        def _():
            forward(1, 1)

        @pl.when(s == 2)
        def _():
            forward(1, 2)

        @pl.when(s == 4)
        def _():
            forward(2, 1)
            forward(2, 2)

        return carry

    lax.fori_loop(0, (rows_tok // tall) * cols, branch, 0)

    weights[4].wait()
    for f in range(3):
        for group in range(len(GROUP)):
            for oc in OFFS:
                for part in range(3):
                    c_copy(f, group, oc, part).wait_recv()

    heads_rows = n_heads * PLEN
    ones = jnp.ones((per_block * PLEN, HD), BF)

    def attend(b):
        keys, values = [], []
        for j in range(per_block):
            first, second, third = [
                final[f][s_slots[f, 0, b * per_block + j]] for f in range(3)
            ]
            keys += [first[0:32], second[0:32]]
            values += [third, first[32:40], second[32:40]]
        keys = jnp.concatenate(keys, axis=0)
        values = jnp.concatenate([jnp.concatenate(values, axis=0), ones], axis=1)
        q = v_q[b].reshape(heads_rows, HD)
        scores = lax.dot_general(q, keys, (((1,), (1,)), ((), ())), preferred_element_type=F32)
        top = jnp.max(scores, axis=-1, keepdims=True)
        weight = jnp.exp(scores - top).astype(BF)
        value = jnp.dot(weight, values, preferred_element_type=F32)
        value = (value[:, :HD] / value[:, HD:]).astype(BF)
        at = pl.ds(b * PLEN, PLEN)
        for h in range(n_heads):
            v_att[at, pl.ds(h * HD, HD)] = value[h * PLEN : (h + 1) * PLEN]

    def att_copy(i):
        return pltpu.make_async_remote_copy(
            src_ref=v_att.at[pl.ds(i * chunk, chunk)],
            dst_ref=v_attp.at[pl.ds(i * chunk, chunk)],
            send_sem=att_ss.at[i],
            recv_sem=att_rs.at[i],
            device_id=(st, other),
            device_id_type=MESH,
        )

    n_chunks = rows_tok // chunk

    def attend_chunk(i, carry):
        per = n_blocks // n_chunks
        for k in range(per):
            attend(i * per + k)
        att_copy(i).start()
        return carry

    lax.fori_loop(0, n_chunks, attend_chunk, 0)

    mine = v_att.shape[1]

    def out_copy(i):
        at = pl.ds(i * chunk, chunk)
        return pltpu.make_async_copy(v_out.at[at], out.at[at], out_sem.at[i])

    def project(i, carry):
        at = pl.ds(pl.multiple_of(i * chunk, chunk), chunk)
        att_copy(i).wait_recv()
        cross = jnp.dot(
            v_att[at, :], v_wout[pl.ds(pl.multiple_of(tp * mine, mine), mine), :], preferred_element_type=F32
        )
        cross = cross + jnp.dot(
            v_attp[at, :],
            v_wout[pl.ds(pl.multiple_of(other * mine, mine), mine), :],
            preferred_element_type=F32,
        )
        v_out[at, :] = (v_conv[at, :] + jax.nn.sigmoid(gate_logit[...]) * cross).astype(BF)
        out_copy(i).start()
        return carry

    lax.fori_loop(0, n_chunks, project, 0)

    for i in range(n_chunks):
        out_copy(i).wait()
        att_copy(i).wait_send()
    for f in range(3):
        for o in OFFS:
            ask_first(f, o).wait_send()
            ask_second(f, o).wait_send()
    tok_remote.wait_send()
    for f in range(3):
        for o in OFFS:
            for p in range(4):
                a_copy(f, o, p).wait_send()
        for group in range(len(GROUP)):
            for ob in OFFS:
                b_copy(f, group, ob).wait_send()
            for oc in OFFS:
                for part in range(3):
                    c_copy(f, group, oc, part).wait_send()


def settle_kernel(mixed, out, held, sems):
    pieces = sems.shape[1]
    rows = mixed.shape[0] // pieces

    def copies(i):
        at = pl.ds(i * rows, rows)
        return (
            pltpu.make_async_copy(mixed.at[at], held.at[at], sems.at[0, i]),
            pltpu.make_async_copy(held.at[at], out.at[at], sems.at[1, i]),
        )

    for i in range(pieces):
        copies(i)[0].start()
    for i in range(pieces):
        copies(i)[0].wait()
        copies(i)[1].start()
    for i in range(pieces):
        copies(i)[1].wait()


def on_device(
    tokens,
    norm_gain,
    branch_outer,
    branch_gate,
    branch_input,
    conv_taps,
    query_weight,
    query_gain,
    head_scale,
    store,
    store_gain,
    key_weight,
    value_weight,
    key_gain,
    out_weight,
    gate_logit,
    passage_ids,
):
    n_pass, plen, width = store.shape
    n_tok, half = tokens.shape
    heads = head_scale.shape[0]
    n_st = lax.axis_size("st")
    blocks = passage_ids.shape[0]

    vmem = pl.BlockSpec(memory_space=pltpu.VMEM)
    smem = pl.BlockSpec(memory_space=pltpu.SMEM)
    hbm = pl.BlockSpec(memory_space=pl.ANY)
    dma = pltpu.SemaphoreType.DMA
    scratch = [
        pltpu.VMEM((n_pass * plen, width), BF),
        pltpu.VMEM((width, 2 * HD), BF),
        pltpu.VMEM((256, width), BF),
        pltpu.VMEM((2, n_tok, half), BF),
        pltpu.VMEM((n_tok, width), BF),
        pltpu.VMEM(branch_outer.shape, BF),
        pltpu.VMEM(branch_gate.shape, BF),
        pltpu.VMEM(branch_input.shape, BF),
        pltpu.VMEM(query_weight.shape, BF),
        pltpu.VMEM(out_weight.shape, BF),
        pltpu.VMEM((blocks, heads, plen, HD), BF),
        pltpu.VMEM((n_tok, half), F32),
        pltpu.VMEM((n_tok, heads * HD), BF),
        pltpu.VMEM((n_tok, heads * HD), BF),
        pltpu.VMEM((n_tok, half), BF),
        pltpu.VMEM((3, RING, RING, 1, n_st * CAP), jnp.int32),
        pltpu.SMEM((3, RING, 1, n_st * CAP), jnp.int32),
        pltpu.SMEM((3, RING, RING, 1, n_st * CAP), jnp.int32),
        pltpu.VMEM((n_st * CAP, n_st * CAP), jnp.int32),
        pltpu.VMEM((3, 1, n_st * CAP), jnp.int32),
        pltpu.SMEM((3, 1, n_st * CAP), jnp.int32),
    ]
    for f in range(3):
        scratch += [pltpu.VMEM((n_pass, ROWS[f], HD), BF)] * RING
    for f in range(3):
        scratch += [pltpu.VMEM((RING, RING, len(g) * CAP, ROWS[f], HD), BF) for g in GROUP]
    for f in range(3):
        scratch += [pltpu.VMEM((RING, 3 * len(g) * CAP, ROWS[f], HD), BF) for g in GROUP]
    for f in range(3):
        scratch += [pltpu.VMEM((n_st * CAP, ROWS[f], HD), BF)]
    scratch += [
        dma((11,)),
        dma((4,)),
        dma((4,)),
        dma((3, 6)),
        dma((3, 6)),
        dma,
        dma,
        dma((9, 4)),
        dma((9, 4)),
        dma((27,)),
        dma((27,)),
        dma((81,)),
        dma((81,)),
        dma((4,)),
        dma((4,)),
    ]
    mixed = pl.pallas_call(
        kernel,
        out_shape=jax.ShapeDtypeStruct((n_tok, half), BF),
        in_specs=[
            smem,
            hbm,
            vmem,
            hbm,
            hbm,
            hbm,
            vmem,
            hbm,
            vmem,
            smem,
            hbm,
            vmem,
            hbm,
            hbm,
            vmem,
            hbm,
            vmem,
        ],
        out_specs=hbm,
        scratch_shapes=scratch,
        compiler_params=pltpu.CompilerParams(
            collective_id=0, has_side_effects=True, vmem_limit_bytes=56 * 1024 * 1024
        ),
    )(
        passage_ids.T,
        tokens,
        norm_gain.reshape(1, -1),
        branch_outer,
        branch_gate,
        branch_input,
        conv_taps,
        query_weight,
        query_gain.reshape(1, -1),
        head_scale,
        store.reshape(n_pass * plen, width),
        store_gain.reshape(1, -1),
        key_weight,
        value_weight,
        key_gain.reshape(1, -1),
        out_weight,
        gate_logit.reshape(1, -1),
    )
    pieces = 8
    return pl.pallas_call(
        settle_kernel,
        out_shape=jax.ShapeDtypeStruct((n_tok, half), BF),
        in_specs=[hbm],
        out_specs=hbm,
        scratch_shapes=[pltpu.VMEM((n_tok, half), BF), dma((2, pieces))],
        compiler_params=pltpu.CompilerParams(vmem_limit_bytes=62 * 1024 * 1024),
    )(mixed)


def solution(mesh):
    return jax.shard_map(
        on_device,
        mesh=mesh,
        in_specs=(
            P("st", "tp"),
            P(),
            P(None, "tp"),
            P(None, "tp"),
            P(None, "tp"),
            P(None, "tp"),
            P(None, "tp"),
            P(),
            P("tp"),
            P("st", None, None),
            P(),
            P(None, "tp"),
            P(None, "tp"),
            P(),
            P(None, "tp"),
            P("tp"),
            P("st", None),
        ),
        out_specs=P("st", "tp"),
        check_vma=False,
    )
```

```python
import math

import jax
import jax.numpy as jnp
from jax import lax
from jax.experimental import pallas as pl
from jax.experimental.pallas import tpu as pltpu
from jax.sharding import PartitionSpec as P

MESH = pl.DeviceIdType.MESH
EPS = 1e-06
SEQ = 128
RING = 4
CAP = 2
HD = 128
PLEN = 64
BF = jnp.bfloat16
F32 = jnp.float32

ORDERS = (("z", "y", "x"), ("y", "x", "z"), ("x", "z", "y"))
ROWS = (40, 40, 48)
STRIDE = {"z": RING * RING, "y": RING, "x": 1}
GROUP = ((0,), (1, 3), (2,))
START = (0, RING * RING * CAP, RING * RING * CAP * 3)
OFFS = (2, 1, 3)
PLACE = {0: 0, 1: 1, 3: 2, 2: 3}
PARTS = ((0,), (1, 3), (2,))


def coordinates(st):
    return {"z": st // 16, "y": lax.rem(st // 4, 4), "x": lax.rem(st, 4)}


def shifted(st, moves):
    at = coordinates(st)
    out = 0
    for axis in ("z", "y", "x"):
        out = out + lax.rem(at[axis] + (moves.get(axis, 0) % RING), RING) * STRIDE[axis]
    return out


def position(group, oc, ob):
    return START[group] + (oc * RING + PLACE[ob]) * len(GROUP[group]) * CAP


def place(group, ob):
    return (PLACE[ob] - 1) * len(GROUP[group]) * CAP


def kernel(
    ids,
    tokens,
    norm_gain,
    w_outer,
    w_gate,
    w_input,
    taps,
    w_query,
    query_gain,
    head_scale,
    store,
    store_gain,
    w_key,
    w_value,
    key_gain,
    w_out,
    gate_logit,
    out,
    v_store,
    v_wkv,
    v_mem,
    v_x,
    v_n,
    v_wo,
    v_wg,
    v_wi,
    v_wq,
    v_wout,
    v_q,
    v_conv,
    v_att,
    v_attp,
    v_out,
    v_ask,
    s_near,
    s_ask,
    v_put,
    v_slots,
    s_slots,
    *rest,
):
    table = [rest[f * 4 : f * 4 + 4] for f in range(3)]
    rest = rest[12:]
    packed = [rest[f * 3 : f * 3 + 3] for f in range(3)]
    rest = rest[9:]
    relay = [rest[f * 3 : f * 3 + 3] for f in range(3)]
    rest = rest[9:]
    final = rest[:3]
    (
        local_sem,
        store_sem,
        out_sem,
        ask_ss,
        ask_rs,
        tok_ss,
        tok_rs,
        a_ss,
        a_rs,
        b_ss,
        b_rs,
        c_ss,
        c_rs,
        att_ss,
        att_rs,
    ) = rest[3:]

    st = lax.axis_index("st")
    tp = lax.axis_index("tp")
    other = 1 - tp
    rows_tok = tokens.shape[0]
    half = tokens.shape[1]
    width = 2 * half
    n_pass = store.shape[0] // PLEN

    store_copies = []
    wk = pltpu.make_async_copy(w_key, v_wkv.at[:, pl.ds(0, HD)], local_sem.at[0])
    wv = pltpu.make_async_copy(w_value, v_wkv.at[:, pl.ds(HD, HD)], local_sem.at[1])
    chunk = 256
    for p in range(4):
        store_copies.append(
            pltpu.make_async_copy(
                store.at[pl.ds(p * chunk, chunk)], v_store.at[pl.ds(p * chunk, chunk)], store_sem.at[p]
            )
        )
    store_copies[0].start()
    wk.start()
    wv.start()
    for p in range(1, 4):
        store_copies[p].start()
    tok_local = pltpu.make_async_copy(tokens, v_x.at[tp], local_sem.at[2])
    tok_local.start()
    weights = []
    for i, (src, dst) in enumerate(
        ((w_query, v_wq), (w_outer, v_wo), (w_gate, v_wg), (w_input, v_wi), (w_out, v_wout))
    ):
        cp = pltpu.make_async_copy(src, dst, local_sem.at[3 + i])
        cp.start()
        weights.append(cp)

    barrier = pltpu.get_barrier_semaphore()
    for axis in STRIDE:
        for o in OFFS:
            pl.semaphore_signal(barrier, inc=1, device_id=(shifted(st, {axis: o}), tp), device_id_type=MESH)
    pl.semaphore_signal(barrier, inc=1, device_id=(st, other), device_id_type=MESH)

    lanes = v_put.shape[1]
    lane = lax.broadcasted_iota(jnp.int32, (1, lanes), 1)
    lane_owner = lane // CAP
    lane_rank = lax.rem(lane, CAP)
    per_block, n_blocks = ids.shape
    v_put[...] = jnp.zeros_like(v_put)

    def request(j, carry):
        wanted, count = carry
        for p in range(per_block):
            number = ids[p, j]
            owner = lax.div(number, n_pass)
            match = lane_owner == owner
            put = match & (count == lane_rank)
            wanted = jnp.where(put, number - owner * n_pass, wanted)
            count = count + match.astype(jnp.int32)
            v_put[pl.ds(j * per_block + p, 1), :] = put.astype(jnp.int32)
        return wanted, count

    zero = jnp.zeros((1, lanes), jnp.int32)
    wanted, _ = lax.fori_loop(0, n_blocks, request, (zero, zero), unroll=4)
    for f in range(3):
        v_ask[f, 0, 0] = wanted
    me = coordinates(st)
    them = {
        "z": lane_owner // (RING * RING),
        "y": lax.rem(lane_owner // RING, RING),
        "x": lax.rem(lane_owner, RING),
    }
    for f in range(3):
        oa, ob, oc = [lax.rem(me[axis] - them[axis] + RING, RING) for axis in ORDERS[f]]
        spot = oc * RING + jnp.where(ob == 2, 3, jnp.where(ob == 3, 2, ob))
        where = jnp.zeros_like(lane)
        for group, members in enumerate(GROUP):
            for j, o in enumerate(members):
                first = START[group] + spot * (len(members) * CAP) + j * CAP
                where = jnp.where(oa == o, first + lane_rank, where)
        spots = v_put[...] * where
        v_slots[f] = jnp.sum(spots.T, axis=0, keepdims=True)

    def ask_first(f, oc):
        return pltpu.make_async_remote_copy(
            src_ref=v_ask.at[f, 0, 0],
            dst_ref=v_ask.at[f, 0, oc],
            send_sem=ask_ss.at[f, oc - 1],
            recv_sem=ask_rs.at[f, oc - 1],
            device_id=(shifted(st, {ORDERS[f][2]: -oc}), tp),
            device_id_type=MESH,
        )

    def ask_second(f, ob):
        return pltpu.make_async_remote_copy(
            src_ref=v_ask.at[f, 0],
            dst_ref=v_ask.at[f, ob],
            send_sem=ask_ss.at[f, 2 + ob],
            recv_sem=ask_rs.at[f, 2 + ob],
            device_id=(shifted(st, {ORDERS[f][1]: -ob}), tp),
            device_id_type=MESH,
        )

    tok_remote = pltpu.make_async_remote_copy(
        src_ref=tokens,
        dst_ref=v_x.at[tp],
        send_sem=tok_ss,
        recv_sem=tok_rs,
        device_id=(st, other),
        device_id_type=MESH,
    )

    def a_copy(f, o, p):
        ahead = o == 1 or (o == 2 and p < 2)
        src = table[f][0] if o != 2 else table[f][1 if ahead else 3]
        return a_step(f, o, p, src, 1 if ahead else 3)

    def a_step(f, o, p, src, move):
        return pltpu.make_async_remote_copy(
            src_ref=src.at[pl.ds(p * 4, 4)],
            dst_ref=table[f][o].at[pl.ds(p * 4, 4)],
            send_sem=a_ss.at[f * 3 + o - 1, p],
            recv_sem=a_rs.at[f * 3 + o - 1, p],
            device_id=(shifted(st, {ORDERS[f][0]: move}), tp),
            device_id_type=MESH,
        )

    wk.wait()
    wv.wait()
    sub = 32

    def kv_chunk(p, carry):
        base = p * chunk
        pltpu.make_async_copy(
            store.at[pl.ds(base, chunk)], v_store.at[pl.ds(base, chunk)], store_sem.at[p]
        ).wait()

        def norm_sub(i, c):
            x = v_store[pl.ds(base + i * sub, sub), :].astype(F32)
            r = lax.rsqrt(jnp.mean(x * x, axis=-1, keepdims=True) + EPS)
            v_mem[pl.ds(i * sub, sub), :] = (x * r * store_gain[...]).astype(BF)
            return c

        lax.fori_loop(0, chunk // sub, norm_sub, 0, unroll=2)
        kv = jnp.dot(v_mem[...], v_wkv[...], preferred_element_type=F32)
        k = kv[:, :HD]
        k = k * lax.rsqrt(jnp.mean(k * k, axis=-1, keepdims=True) + EPS) * key_gain[...]
        k = k.astype(BF).reshape(4, PLEN, HD)
        v = kv[:, HD:].astype(BF).reshape(4, PLEN, HD)
        at = pl.ds(p * 4, 4)
        table[0][0][at, 0:32, :] = k[:, 0:32]
        table[0][0][at, 32:40, :] = v[:, 48:56]
        table[1][0][at, 0:32, :] = k[:, 32:64]
        table[1][0][at, 32:40, :] = v[:, 56:64]
        table[2][0][at, :, :] = v[:, 0:48]

        @pl.when(p == 0)
        def _():
            pl.semaphore_wait(barrier, 3 * len(OFFS) + 1)
            for f in range(3):
                for oc in OFFS:
                    ask_first(f, oc).start()

        @pl.when(p == 3)
        def _():
            for f in range(3):
                for oc in OFFS:
                    ask_first(f, oc).wait_recv()
            for f in range(3):
                for ob in OFFS:
                    ask_second(f, ob).start()

        for f in range(3):
            for o in (1, 3):
                a_step(f, o, p, table[f][0], o).start()

        @pl.when(p == 0)
        def _():
            tok_remote.start()

        return carry

    lax.fori_loop(0, 4, kv_chunk, 0)

    def pack(group, near):
        n = len(GROUP[group]) * CAP
        for f in range(3):
            owners = [shifted(st, {ORDERS[f][0]: -o}) for o in GROUP[group]]

            def one(t, carry, f=f, owners=owners):
                ob = 0 if near else 1 + t // RING
                oc = lax.rem(t, RING)
                for j, o in enumerate(GROUP[group]):
                    for r in range(CAP):
                        lane_at = owners[j] * CAP + r
                        at = s_near[f, oc, 0, lane_at] if near else s_ask[f, ob, oc, 0, lane_at]
                        packed[f][group][ob, oc, j * CAP + r] = table[f][o][at]
                return carry

            lax.fori_loop(0, RING * (1 if near else RING - 1), one, 0, unroll=2)
            if near:
                final[f][pl.ds(position(group, 0, 0), n)] = packed[f][group][0, 0]

    def b_copy(f, group, ob):
        i = (f * 3 + group) * 3 + ob - 1
        return pltpu.make_async_remote_copy(
            src_ref=packed[f][group].at[ob],
            dst_ref=relay[f][group].at[:, pl.ds(place(group, ob), len(GROUP[group]) * CAP)],
            send_sem=b_ss.at[i],
            recv_sem=b_rs.at[i],
            device_id=(shifted(st, {ORDERS[f][1]: ob}), tp),
            device_id_type=MESH,
        )

    def c_copy(f, group, oc, part):
        obs = PARTS[part]
        n = len(GROUP[group]) * CAP * len(obs)
        i = ((f * 3 + group) * 3 + oc - 1) * 3 + part
        if part == 0:
            src = packed[f][group].at[0, oc]
        else:
            src = relay[f][group].at[oc, pl.ds(place(group, obs[0]), n)]
        return pltpu.make_async_remote_copy(
            src_ref=src,
            dst_ref=final[f].at[pl.ds(position(group, oc, obs[0]), n)],
            send_sem=c_ss.at[i],
            recv_sem=c_rs.at[i],
            device_id=(shifted(st, {ORDERS[f][2]: oc}), tp),
            device_id_type=MESH,
        )

    def send_packed(group):
        for f in range(3):
            for ob in OFFS:
                b_copy(f, group, ob).start()

    def send_near(group):
        for f in range(3):
            for oc in OFFS:
                c_copy(f, group, oc, 0).start()

    def forward(group, part):
        n = len(GROUP[group]) * CAP
        for f in range(3):
            for ob in PARTS[part]:
                b_copy(f, group, ob).wait_recv()
            for oc in OFFS:
                c_copy(f, group, oc, part).start()
            for ob in PARTS[part]:
                final[f][pl.ds(position(group, 0, ob), n)] = relay[f][group][0, pl.ds(place(group, ob), n)]

    tok_local.wait()

    def norm_tok(i, c):
        at = pl.ds(i * sub, sub)
        x0 = v_x[0, at, :].astype(F32)
        x1 = v_x[1, at, :].astype(F32)
        total = jnp.sum(x0 * x0, axis=-1, keepdims=True) + jnp.sum(x1 * x1, axis=-1, keepdims=True)
        r = lax.rsqrt(total * (1.0 / width) + EPS)
        v_n[at, pl.ds(0, half)] = (x0 * r * norm_gain[:, 0:half]).astype(BF)
        v_n[at, pl.ds(half, half)] = (x1 * r * norm_gain[:, half:width]).astype(BF)
        return c

    near_local = pltpu.make_async_copy(v_ask.at[:, 0], s_near, local_sem.at[8])
    near_local.start()
    slots_local = pltpu.make_async_copy(v_slots, s_slots, local_sem.at[9])
    slots_local.start()
    tok_remote.wait_recv()
    n_sub = rows_tok // sub
    quarter = n_sub // 4
    lax.fori_loop(0, quarter, norm_tok, 0, unroll=2)
    near_local.wait()
    slots_local.wait()
    pack(0, True)
    send_near(0)

    def onward(p):
        for f in range(3):
            a_copy(f, 1 if p < 2 else 3, p).wait_recv()
            a_copy(f, 2, p).start()

    onward(0)
    onward(1)
    lax.fori_loop(quarter, 2 * quarter, norm_tok, 0, unroll=2)
    onward(2)
    onward(3)
    for f in range(3):
        for p in range(4):
            a_copy(f, 3 if p < 2 else 1, p).wait_recv()
    pack(1, True)
    send_near(1)
    for f in range(3):
        for ob in OFFS:
            ask_second(f, ob).wait_recv()
    ask_local = pltpu.make_async_copy(v_ask, s_ask, local_sem.at[10])
    ask_local.start()
    ask_local.wait()
    for group in range(2):
        pack(group, False)
        send_packed(group)
    lax.fori_loop(2 * quarter, n_sub, norm_tok, 0, unroll=2)
    for f in range(3):
        for p in range(4):
            a_copy(f, 2, p).wait_recv()
    pack(2, False)
    send_packed(2)
    pack(2, True)
    send_near(2)

    weights[0].wait()
    n_heads = v_q.shape[1]

    def query_chunk(i, c):
        raw = jnp.dot(v_n[pl.ds(i * chunk, chunk), :], v_wq[...], preferred_element_type=F32)
        for h in range(n_heads):
            q = raw[:, h * HD : (h + 1) * HD]
            q = q * lax.rsqrt(jnp.mean(q * q, axis=-1, keepdims=True) + EPS) * query_gain[...]
            q = (q * (head_scale[h] / math.sqrt(HD))).astype(BF).reshape(chunk // PLEN, PLEN, HD)
            v_q[pl.ds(i * (chunk // PLEN), chunk // PLEN), h] = q
        return c

    lax.fori_loop(0, rows_tok // chunk, query_chunk, 0)

    for cp in weights[1:4]:
        cp.wait()
    tall, wide = 512, 256
    cols = v_wo.shape[1] // wide

    def branch(s, carry):
        rows = pl.ds(pl.multiple_of((s // cols) * tall, tall), tall)
        at = pl.ds(pl.multiple_of(lax.rem(s, cols) * wide, wide), wide)
        n = v_n[rows, :]
        gate = jnp.dot(n, v_wg[:, at], preferred_element_type=F32)
        z = gate * jnp.dot(n, v_wi[:, at], preferred_element_type=F32)
        row = lax.rem(lax.broadcasted_iota(jnp.int32, (tall, wide), 0), SEQ)
        one = jnp.where(row >= 1, pltpu.roll(z, 1, 0), 0.0)
        two = jnp.where(row >= 2, pltpu.roll(z, 2, 0), 0.0)
        t = taps[:, at]
        conv = two * t[0:1] + one * t[1:2] + z * t[2:3]
        v_conv[rows, at] = conv
        v_conv[rows, at] = (
            jnp.dot(n, v_wo[:, at], preferred_element_type=F32) * v_conv[rows, at]
        )

        @pl.when(s == 0)
        def _():
            forward(0, 2)
            forward(0, 1)

        @pl.when(s == 1)
        def _():
            forward(1, 2)

        @pl.when(s == 2)
        def _():
            forward(1, 1)

        @pl.when(s == 4)
        def _():
            forward(2, 2)
            forward(2, 1)

        return carry

    lax.fori_loop(0, (rows_tok // tall) * cols, branch, 0)

    weights[4].wait()
    for f in range(3):
        for o in OFFS:
            ask_first(f, o).wait_send()
            ask_second(f, o).wait_send()
            for p in range(4):
                a_copy(f, o, p).wait_send()
            for group in range(len(GROUP)):
                b_copy(f, group, o).wait_send()
    tok_remote.wait_send()
    for group in range(len(GROUP)):
        for part in range(3):
            part = (0, 2, 1)[part]
            arriving = [c_copy(f, group, oc, part) for f in range(3) for oc in OFFS]
            for cp in arriving:
                cp.wait_send()
            for cp in arriving:
                cp.wait_recv()

    heads_rows = n_heads * PLEN
    ones = jnp.ones((per_block * PLEN, HD), BF)

    def attend(b):
        keys, values = [], []
        for j in range(per_block):
            first, second, third = [
                final[f][s_slots[f, 0, b * per_block + j]] for f in range(3)
            ]
            keys += [first[0:32], second[0:32]]
            values += [third, first[32:40], second[32:40]]
        keys = jnp.concatenate(keys, axis=0)
        values = jnp.concatenate([jnp.concatenate(values, axis=0), ones], axis=1)
        q = v_q[b].reshape(heads_rows, HD)
        scores = lax.dot_general(q, keys, (((1,), (1,)), ((), ())), preferred_element_type=F32)
        top = jnp.max(scores, axis=-1, keepdims=True)
        weight = jnp.exp(scores - top).astype(BF)
        value = jnp.dot(weight, values, preferred_element_type=F32)
        value = (value[:, :HD] / value[:, HD:]).astype(BF)
        at = pl.ds(b * PLEN, PLEN)
        for h in range(n_heads):
            v_att[at, pl.ds(h * HD, HD)] = value[h * PLEN : (h + 1) * PLEN]

    def att_copy(i):
        return pltpu.make_async_remote_copy(
            src_ref=v_att.at[pl.ds(i * chunk, chunk)],
            dst_ref=v_attp.at[pl.ds(i * chunk, chunk)],
            send_sem=att_ss.at[i],
            recv_sem=att_rs.at[i],
            device_id=(st, other),
            device_id_type=MESH,
        )

    n_chunks = rows_tok // chunk

    def attend_chunk(i, carry):
        per = n_blocks // n_chunks
        for k in range(per):
            attend(i * per + k)
        att_copy(i).start()
        return carry

    lax.fori_loop(0, n_chunks, attend_chunk, 0)

    mine = v_att.shape[1]

    def out_copy(i):
        at = pl.ds(i * chunk, chunk)
        return pltpu.make_async_copy(v_out.at[at], out.at[at], out_sem.at[i])

    def project(i, carry):
        at = pl.ds(pl.multiple_of(i * chunk, chunk), chunk)
        att_copy(i).wait_recv()
        cross = jnp.dot(
            v_att[at, :], v_wout[pl.ds(pl.multiple_of(tp * mine, mine), mine), :], preferred_element_type=F32
        )
        cross = cross + jnp.dot(
            v_attp[at, :],
            v_wout[pl.ds(pl.multiple_of(other * mine, mine), mine), :],
            preferred_element_type=F32,
        )
        v_out[at, :] = (v_conv[at, :] + jax.nn.sigmoid(gate_logit[...]) * cross).astype(BF)
        out_copy(i).start()
        return carry

    lax.fori_loop(0, n_chunks, project, 0)

    for i in range(n_chunks):
        out_copy(i).wait()
        att_copy(i).wait_send()


def settle_kernel(mixed, out, held, sems):
    pieces = sems.shape[1]
    rows = mixed.shape[0] // pieces

    def copies(i):
        at = pl.ds(i * rows, rows)
        return (
            pltpu.make_async_copy(mixed.at[at], held.at[at], sems.at[0, i]),
            pltpu.make_async_copy(held.at[at], out.at[at], sems.at[1, i]),
        )

    for i in range(pieces):
        copies(i)[0].start()
    for i in range(pieces):
        copies(i)[0].wait()
        copies(i)[1].start()
    for i in range(pieces):
        copies(i)[1].wait()


def on_device(
    tokens,
    norm_gain,
    branch_outer,
    branch_gate,
    branch_input,
    conv_taps,
    query_weight,
    query_gain,
    head_scale,
    store,
    store_gain,
    key_weight,
    value_weight,
    key_gain,
    out_weight,
    gate_logit,
    passage_ids,
):
    n_pass, plen, width = store.shape
    n_tok, half = tokens.shape
    heads = head_scale.shape[0]
    n_st = lax.axis_size("st")
    blocks = passage_ids.shape[0]

    vmem = pl.BlockSpec(memory_space=pltpu.VMEM)
    smem = pl.BlockSpec(memory_space=pltpu.SMEM)
    hbm = pl.BlockSpec(memory_space=pl.ANY)
    dma = pltpu.SemaphoreType.DMA
    scratch = [
        pltpu.VMEM((n_pass * plen, width), BF),
        pltpu.VMEM((width, 2 * HD), BF),
        pltpu.VMEM((256, width), BF),
        pltpu.VMEM((2, n_tok, half), BF),
        pltpu.VMEM((n_tok, width), BF),
        pltpu.VMEM(branch_outer.shape, BF),
        pltpu.VMEM(branch_gate.shape, BF),
        pltpu.VMEM(branch_input.shape, BF),
        pltpu.VMEM(query_weight.shape, BF),
        pltpu.VMEM(out_weight.shape, BF),
        pltpu.VMEM((blocks, heads, plen, HD), BF),
        pltpu.VMEM((n_tok, half), F32),
        pltpu.VMEM((n_tok, heads * HD), BF),
        pltpu.VMEM((n_tok, heads * HD), BF),
        pltpu.VMEM((n_tok, half), BF),
        pltpu.VMEM((3, RING, RING, 1, n_st * CAP), jnp.int32),
        pltpu.SMEM((3, RING, 1, n_st * CAP), jnp.int32),
        pltpu.SMEM((3, RING, RING, 1, n_st * CAP), jnp.int32),
        pltpu.VMEM((n_st * CAP, n_st * CAP), jnp.int32),
        pltpu.VMEM((3, 1, n_st * CAP), jnp.int32),
        pltpu.SMEM((3, 1, n_st * CAP), jnp.int32),
    ]
    for f in range(3):
        scratch += [pltpu.VMEM((n_pass, ROWS[f], HD), BF)] * RING
    for f in range(3):
        scratch += [pltpu.VMEM((RING, RING, len(g) * CAP, ROWS[f], HD), BF) for g in GROUP]
    for f in range(3):
        scratch += [pltpu.VMEM((RING, 3 * len(g) * CAP, ROWS[f], HD), BF) for g in GROUP]
    for f in range(3):
        scratch += [pltpu.VMEM((n_st * CAP, ROWS[f], HD), BF)]
    scratch += [
        dma((11,)),
        dma((4,)),
        dma((4,)),
        dma((3, 6)),
        dma((3, 6)),
        dma,
        dma,
        dma((9, 4)),
        dma((9, 4)),
        dma((27,)),
        dma((27,)),
        dma((81,)),
        dma((81,)),
        dma((4,)),
        dma((4,)),
    ]
    mixed = pl.pallas_call(
        kernel,
        out_shape=jax.ShapeDtypeStruct((n_tok, half), BF),
        in_specs=[
            smem,
            hbm,
            vmem,
            hbm,
            hbm,
            hbm,
            vmem,
            hbm,
            vmem,
            smem,
            hbm,
            vmem,
            hbm,
            hbm,
            vmem,
            hbm,
            vmem,
        ],
        out_specs=hbm,
        scratch_shapes=scratch,
        compiler_params=pltpu.CompilerParams(
            collective_id=0, has_side_effects=True, vmem_limit_bytes=56 * 1024 * 1024
        ),
    )(
        passage_ids.T,
        tokens,
        norm_gain.reshape(1, -1),
        branch_outer,
        branch_gate,
        branch_input,
        conv_taps,
        query_weight,
        query_gain.reshape(1, -1),
        head_scale,
        store.reshape(n_pass * plen, width),
        store_gain.reshape(1, -1),
        key_weight,
        value_weight,
        key_gain.reshape(1, -1),
        out_weight,
        gate_logit.reshape(1, -1),
    )
    pieces = 8
    return pl.pallas_call(
        settle_kernel,
        out_shape=jax.ShapeDtypeStruct((n_tok, half), BF),
        in_specs=[hbm],
        out_specs=hbm,
        scratch_shapes=[pltpu.VMEM((n_tok, half), BF), dma((2, pieces))],
        compiler_params=pltpu.CompilerParams(vmem_limit_bytes=62 * 1024 * 1024),
    )(mixed)


def solution(mesh):
    return jax.shard_map(
        on_device,
        mesh=mesh,
        in_specs=(
            P("st", "tp"),
            P(),
            P(None, "tp"),
            P(None, "tp"),
            P(None, "tp"),
            P(None, "tp"),
            P(None, "tp"),
            P(),
            P("tp"),
            P("st", None, None),
            P(),
            P(None, "tp"),
            P(None, "tp"),
            P(),
            P(None, "tp"),
            P("tp"),
            P("st", None),
        ),
        out_specs=P("st", "tp"),
        check_vma=False,
    )
```

```python
import math

import jax
import jax.numpy as jnp
from jax import lax
from jax.experimental import pallas as pl
from jax.experimental.pallas import tpu as pltpu
from jax.sharding import PartitionSpec as P

MESH = pl.DeviceIdType.MESH
EPS = 1e-06
SEQ = 128
RING = 4
CAP = 2
HD = 128
PLEN = 64
BF = jnp.bfloat16
F32 = jnp.float32

ORDERS = (("z", "y", "x"), ("y", "x", "z"), ("x", "z", "y"))
ROWS = (40, 40, 48)
STRIDE = {"z": RING * RING, "y": RING, "x": 1}
GROUP = ((0,), (1, 3), (2,))
START = (0, RING * RING * CAP, RING * RING * CAP * 3)
OFFS = (2, 1, 3)
PLACE = {0: 0, 1: 1, 3: 2, 2: 3}
PARTS = ((0,), (1, 3), (2,))


def coordinates(st):
    return {"z": st // 16, "y": lax.rem(st // 4, 4), "x": lax.rem(st, 4)}


def shifted(st, moves):
    at = coordinates(st)
    out = 0
    for axis in ("z", "y", "x"):
        out = out + lax.rem(at[axis] + (moves.get(axis, 0) % RING), RING) * STRIDE[axis]
    return out


def position(group, oc, ob):
    return START[group] + (oc * RING + PLACE[ob]) * len(GROUP[group]) * CAP


def place(group, ob):
    return (PLACE[ob] - 1) * len(GROUP[group]) * CAP


def kernel(
    ids,
    tokens,
    norm_gain,
    w_outer,
    w_gate,
    w_input,
    taps,
    w_query,
    query_gain,
    head_scale,
    store,
    store_gain,
    w_key,
    w_value,
    key_gain,
    w_out,
    gate_logit,
    out,
    v_store,
    v_wkv,
    v_mem,
    v_x,
    v_n,
    v_wo,
    v_wg,
    v_wi,
    v_wq,
    v_wout,
    v_q,
    v_conv,
    v_att,
    v_out,
    v_ask,
    s_near,
    s_ask,
    v_put,
    v_slots,
    s_slots,
    *rest,
):
    table = [rest[f * 4 : f * 4 + 4] for f in range(3)]
    rest = rest[12:]
    packed = [rest[f * 3 : f * 3 + 3] for f in range(3)]
    rest = rest[9:]
    relay = [rest[f * 3 : f * 3 + 3] for f in range(3)]
    rest = rest[9:]
    final = rest[:3]
    (
        local_sem,
        store_sem,
        out_sem,
        ask_ss,
        ask_rs,
        tok_ss,
        tok_rs,
        a_ss,
        a_rs,
        b_ss,
        b_rs,
        c_ss,
        c_rs,
        att_ss,
        att_rs,
    ) = rest[3:]

    st = lax.axis_index("st")
    tp = lax.axis_index("tp")
    other = 1 - tp
    rows_tok = tokens.shape[0]
    half = tokens.shape[1]
    width = 2 * half
    n_pass = store.shape[0] // PLEN

    store_copies = []
    wk = pltpu.make_async_copy(w_key, v_wkv.at[:, pl.ds(0, HD)], local_sem.at[0])
    wv = pltpu.make_async_copy(w_value, v_wkv.at[:, pl.ds(HD, HD)], local_sem.at[1])
    chunk = 256
    for p in range(4):
        store_copies.append(
            pltpu.make_async_copy(
                store.at[pl.ds(p * chunk, chunk)], v_store.at[pl.ds(p * chunk, chunk)], store_sem.at[p]
            )
        )
    store_copies[0].start()
    wk.start()
    wv.start()
    for p in range(1, 4):
        store_copies[p].start()
    tok_local = pltpu.make_async_copy(tokens, v_x.at[tp], local_sem.at[2])
    tok_local.start()
    weights = []
    for i, (src, dst) in enumerate(
        ((w_query, v_wq), (w_outer, v_wo), (w_gate, v_wg), (w_input, v_wi), (w_out, v_wout))
    ):
        cp = pltpu.make_async_copy(src, dst, local_sem.at[3 + i])
        cp.start()
        weights.append(cp)

    barrier = pltpu.get_barrier_semaphore()
    for axis in STRIDE:
        for o in OFFS:
            pl.semaphore_signal(barrier, inc=1, device_id=(shifted(st, {axis: o}), tp), device_id_type=MESH)
    pl.semaphore_signal(barrier, inc=1, device_id=(st, other), device_id_type=MESH)

    lanes = v_put.shape[1]
    lane = lax.broadcasted_iota(jnp.int32, (1, lanes), 1)
    lane_owner = lane // CAP
    lane_rank = lax.rem(lane, CAP)
    per_block, n_blocks = ids.shape
    v_put[...] = jnp.zeros_like(v_put)

    def request(j, carry):
        wanted, count = carry
        for p in range(per_block):
            number = ids[p, j]
            owner = lax.div(number, n_pass)
            match = lane_owner == owner
            put = match & (count == lane_rank)
            wanted = jnp.where(put, number - owner * n_pass, wanted)
            count = count + match.astype(jnp.int32)
            v_put[pl.ds(j * per_block + p, 1), :] = put.astype(jnp.int32)
        return wanted, count

    zero = jnp.zeros((1, lanes), jnp.int32)
    wanted, _ = lax.fori_loop(0, n_blocks, request, (zero, zero), unroll=4)
    for f in range(3):
        v_ask[f, 0, 0] = wanted
    me = coordinates(st)
    them = {
        "z": lane_owner // (RING * RING),
        "y": lax.rem(lane_owner // RING, RING),
        "x": lax.rem(lane_owner, RING),
    }
    for f in range(3):
        oa, ob, oc = [lax.rem(me[axis] - them[axis] + RING, RING) for axis in ORDERS[f]]
        spot = oc * RING + jnp.where(ob == 2, 3, jnp.where(ob == 3, 2, ob))
        where = jnp.zeros_like(lane)
        for group, members in enumerate(GROUP):
            for j, o in enumerate(members):
                first = START[group] + spot * (len(members) * CAP) + j * CAP
                where = jnp.where(oa == o, first + lane_rank, where)
        spots = v_put[...] * where
        v_slots[f] = jnp.sum(spots.T, axis=0, keepdims=True)

    def ask_first(f, oc):
        return pltpu.make_async_remote_copy(
            src_ref=v_ask.at[f, 0, 0],
            dst_ref=v_ask.at[f, 0, oc],
            send_sem=ask_ss.at[f, oc - 1],
            recv_sem=ask_rs.at[f, oc - 1],
            device_id=(shifted(st, {ORDERS[f][2]: -oc}), tp),
            device_id_type=MESH,
        )

    def ask_second(f, ob):
        return pltpu.make_async_remote_copy(
            src_ref=v_ask.at[f, 0],
            dst_ref=v_ask.at[f, ob],
            send_sem=ask_ss.at[f, 2 + ob],
            recv_sem=ask_rs.at[f, 2 + ob],
            device_id=(shifted(st, {ORDERS[f][1]: -ob}), tp),
            device_id_type=MESH,
        )

    tok_remote = pltpu.make_async_remote_copy(
        src_ref=tokens,
        dst_ref=v_x.at[tp],
        send_sem=tok_ss,
        recv_sem=tok_rs,
        device_id=(st, other),
        device_id_type=MESH,
    )

    def a_copy(f, o, p):
        ahead = o == 1 or (o == 2 and p < 2)
        src = table[f][0] if o != 2 else table[f][1 if ahead else 3]
        return a_step(f, o, p, src, 1 if ahead else 3)

    def a_step(f, o, p, src, move):
        return pltpu.make_async_remote_copy(
            src_ref=src.at[pl.ds(p * 4, 4)],
            dst_ref=table[f][o].at[pl.ds(p * 4, 4)],
            send_sem=a_ss.at[f * 3 + o - 1, p],
            recv_sem=a_rs.at[f * 3 + o - 1, p],
            device_id=(shifted(st, {ORDERS[f][0]: move}), tp),
            device_id_type=MESH,
        )

    wk.wait()
    wv.wait()
    sub = 32

    def kv_chunk(p, carry):
        base = p * chunk
        pltpu.make_async_copy(
            store.at[pl.ds(base, chunk)], v_store.at[pl.ds(base, chunk)], store_sem.at[p]
        ).wait()

        def norm_sub(i, c):
            x = v_store[pl.ds(base + i * sub, sub), :].astype(F32)
            r = lax.rsqrt(jnp.mean(x * x, axis=-1, keepdims=True) + EPS)
            v_mem[pl.ds(i * sub, sub), :] = (x * r * store_gain[...]).astype(BF)
            return c

        lax.fori_loop(0, chunk // sub, norm_sub, 0, unroll=2)
        kv = jnp.dot(v_mem[...], v_wkv[...], preferred_element_type=F32)
        k = kv[:, :HD]
        k = k * lax.rsqrt(jnp.mean(k * k, axis=-1, keepdims=True) + EPS) * key_gain[...]
        k = k.astype(BF).reshape(4, PLEN, HD)
        v = kv[:, HD:].astype(BF).reshape(4, PLEN, HD)
        at = pl.ds(p * 4, 4)
        table[0][0][at, 0:32, :] = k[:, 0:32]
        table[0][0][at, 32:40, :] = v[:, 48:56]
        table[1][0][at, 0:32, :] = k[:, 32:64]
        table[1][0][at, 32:40, :] = v[:, 56:64]
        table[2][0][at, :, :] = v[:, 0:48]

        @pl.when(p == 0)
        def _():
            pl.semaphore_wait(barrier, 3 * len(OFFS) + 1)
            for f in range(3):
                for oc in OFFS:
                    ask_first(f, oc).start()

        @pl.when(p == 3)
        def _():
            for f in range(3):
                for oc in OFFS:
                    ask_first(f, oc).wait_recv()
            for f in range(3):
                for ob in OFFS:
                    ask_second(f, ob).start()

        for f in range(3):
            for o in (1, 3):
                a_step(f, o, p, table[f][0], o).start()

        @pl.when(p == 0)
        def _():
            tok_remote.start()

        return carry

    lax.fori_loop(0, 4, kv_chunk, 0)

    def pack(group, near):
        n = len(GROUP[group]) * CAP
        for f in range(3):
            owners = [shifted(st, {ORDERS[f][0]: -o}) for o in GROUP[group]]

            def one(t, carry, f=f, owners=owners):
                ob = 0 if near else 1 + t // RING
                oc = lax.rem(t, RING)
                for j, o in enumerate(GROUP[group]):
                    for r in range(CAP):
                        lane_at = owners[j] * CAP + r
                        at = s_near[f, oc, 0, lane_at] if near else s_ask[f, ob, oc, 0, lane_at]
                        packed[f][group][ob, oc, j * CAP + r] = table[f][o][at]
                return carry

            lax.fori_loop(0, RING * (1 if near else RING - 1), one, 0, unroll=2)
            if near:
                final[f][pl.ds(position(group, 0, 0), n)] = packed[f][group][0, 0]

    def b_copy(f, group, ob):
        i = (f * 3 + group) * 3 + ob - 1
        return pltpu.make_async_remote_copy(
            src_ref=packed[f][group].at[ob],
            dst_ref=relay[f][group].at[:, pl.ds(place(group, ob), len(GROUP[group]) * CAP)],
            send_sem=b_ss.at[i],
            recv_sem=b_rs.at[i],
            device_id=(shifted(st, {ORDERS[f][1]: ob}), tp),
            device_id_type=MESH,
        )

    def c_copy(f, group, oc, part):
        obs = PARTS[part]
        n = len(GROUP[group]) * CAP * len(obs)
        i = ((f * 3 + group) * 3 + oc - 1) * 3 + part
        if part == 0:
            src = packed[f][group].at[0, oc]
        else:
            src = relay[f][group].at[oc, pl.ds(place(group, obs[0]), n)]
        return pltpu.make_async_remote_copy(
            src_ref=src,
            dst_ref=final[f].at[pl.ds(position(group, oc, obs[0]), n)],
            send_sem=c_ss.at[i],
            recv_sem=c_rs.at[i],
            device_id=(shifted(st, {ORDERS[f][2]: oc}), tp),
            device_id_type=MESH,
        )

    def send_packed(group):
        for f in range(3):
            for ob in OFFS:
                b_copy(f, group, ob).start()

    def send_near(group):
        for f in range(3):
            for oc in OFFS:
                c_copy(f, group, oc, 0).start()

    def forward(group, part):
        n = len(GROUP[group]) * CAP
        for f in range(3):
            for ob in PARTS[part]:
                b_copy(f, group, ob).wait_recv()
            for oc in OFFS:
                c_copy(f, group, oc, part).start()
            for ob in PARTS[part]:
                final[f][pl.ds(position(group, 0, ob), n)] = relay[f][group][0, pl.ds(place(group, ob), n)]

    tok_local.wait()

    def norm_tok(i, c):
        at = pl.ds(i * sub, sub)
        x0 = v_x[0, at, :].astype(F32)
        x1 = v_x[1, at, :].astype(F32)
        total = jnp.sum(x0 * x0, axis=-1, keepdims=True) + jnp.sum(x1 * x1, axis=-1, keepdims=True)
        r = lax.rsqrt(total * (1.0 / width) + EPS)
        v_n[at, pl.ds(0, half)] = (x0 * r * norm_gain[:, 0:half]).astype(BF)
        v_n[at, pl.ds(half, half)] = (x1 * r * norm_gain[:, half:width]).astype(BF)
        return c

    near_local = pltpu.make_async_copy(v_ask.at[:, 0], s_near, local_sem.at[8])
    near_local.start()
    slots_local = pltpu.make_async_copy(v_slots, s_slots, local_sem.at[9])
    slots_local.start()
    tok_remote.wait_recv()
    n_sub = rows_tok // sub
    quarter = n_sub // 4
    lax.fori_loop(0, quarter, norm_tok, 0, unroll=2)
    near_local.wait()
    slots_local.wait()
    pack(0, True)
    send_near(0)

    def onward(p):
        for f in range(3):
            a_copy(f, 1 if p < 2 else 3, p).wait_recv()
            a_copy(f, 2, p).start()

    onward(0)
    onward(1)
    lax.fori_loop(quarter, 2 * quarter, norm_tok, 0, unroll=2)
    onward(2)
    onward(3)
    for f in range(3):
        for p in range(4):
            a_copy(f, 3 if p < 2 else 1, p).wait_recv()
    pack(1, True)
    send_near(1)
    for f in range(3):
        for ob in OFFS:
            ask_second(f, ob).wait_recv()
    ask_local = pltpu.make_async_copy(v_ask, s_ask, local_sem.at[10])
    ask_local.start()
    ask_local.wait()
    for group in range(2):
        pack(group, False)
        send_packed(group)
    lax.fori_loop(2 * quarter, n_sub, norm_tok, 0, unroll=2)
    for f in range(3):
        for p in range(4):
            a_copy(f, 2, p).wait_recv()
    pack(2, False)
    send_packed(2)
    pack(2, True)
    send_near(2)

    weights[0].wait()
    n_heads = v_q.shape[1]

    def query_chunk(i, c):
        raw = jnp.dot(v_n[pl.ds(i * chunk, chunk), :], v_wq[...], preferred_element_type=F32)
        for h in range(n_heads):
            q = raw[:, h * HD : (h + 1) * HD]
            q = q * lax.rsqrt(jnp.mean(q * q, axis=-1, keepdims=True) + EPS) * query_gain[...]
            q = (q * (head_scale[h] / math.sqrt(HD))).astype(BF).reshape(chunk // PLEN, PLEN, HD)
            v_q[pl.ds(i * (chunk // PLEN), chunk // PLEN), h] = q
        return c

    lax.fori_loop(0, rows_tok // chunk, query_chunk, 0)

    for cp in weights[1:4]:
        cp.wait()
    tall, wide = 512, 256
    cols = v_wo.shape[1] // wide

    def branch(s, carry):
        rows = pl.ds(pl.multiple_of((s // cols) * tall, tall), tall)
        at = pl.ds(pl.multiple_of(lax.rem(s, cols) * wide, wide), wide)
        n = v_n[rows, :]
        gate = jnp.dot(n, v_wg[:, at], preferred_element_type=F32)
        z = gate * jnp.dot(n, v_wi[:, at], preferred_element_type=F32)
        row = lax.rem(lax.broadcasted_iota(jnp.int32, (tall, wide), 0), SEQ)
        one = jnp.where(row >= 1, pltpu.roll(z, 1, 0), 0.0)
        two = jnp.where(row >= 2, pltpu.roll(z, 2, 0), 0.0)
        t = taps[:, at]
        conv = two * t[0:1] + one * t[1:2] + z * t[2:3]
        v_conv[rows, at] = conv
        v_conv[rows, at] = (
            jnp.dot(n, v_wo[:, at], preferred_element_type=F32) * v_conv[rows, at]
        )

        @pl.when(s == 0)
        def _():
            forward(0, 2)
            forward(0, 1)

        @pl.when(s == 1)
        def _():
            forward(1, 2)

        @pl.when(s == 2)
        def _():
            forward(1, 1)

        @pl.when(s == 4)
        def _():
            forward(2, 2)
            forward(2, 1)

        return carry

    lax.fori_loop(0, (rows_tok // tall) * cols, branch, 0)

    weights[4].wait()
    for f in range(3):
        for o in OFFS:
            ask_first(f, o).wait_send()
            ask_second(f, o).wait_send()
            for p in range(4):
                a_copy(f, o, p).wait_send()
            for group in range(len(GROUP)):
                b_copy(f, group, o).wait_send()
    tok_remote.wait_send()
    for group in range(len(GROUP)):
        for part in range(3):
            part = (0, 2, 1)[part]
            arriving = [c_copy(f, group, oc, part) for f in range(3) for oc in OFFS]
            for cp in arriving:
                cp.wait_send()
            for cp in arriving:
                cp.wait_recv()

    heads_rows = n_heads * PLEN
    heads_width = n_heads * HD
    own_cols = pl.ds(pl.multiple_of(tp * heads_width, heads_width), heads_width)
    ones = jnp.ones((per_block * PLEN, HD), BF)

    def attend(b):
        keys, values = [], []
        for j in range(per_block):
            first, second, third = [
                final[f][s_slots[f, 0, b * per_block + j]] for f in range(3)
            ]
            keys += [first[0:32], second[0:32]]
            values += [third, first[32:40], second[32:40]]
        keys = jnp.concatenate(keys, axis=0)
        values = jnp.concatenate([jnp.concatenate(values, axis=0), ones], axis=1)
        q = v_q[b].reshape(heads_rows, HD)
        scores = lax.dot_general(q, keys, (((1,), (1,)), ((), ())), preferred_element_type=F32)
        top = jnp.max(scores, axis=-1, keepdims=True)
        weight = jnp.exp(scores - top).astype(BF)
        value = jnp.dot(weight, values, preferred_element_type=F32)
        value = (value[:, :HD] / value[:, HD:]).astype(BF)
        at = pl.ds(b * PLEN, PLEN)
        for h in range(n_heads):
            v_att[at, pl.ds(pl.multiple_of(tp * heads_width + h * HD, HD), HD)] = value[h * PLEN : (h + 1) * PLEN]

    def att_copy(i):
        return pltpu.make_async_remote_copy(
            src_ref=v_att.at[pl.ds(i * chunk, chunk), own_cols],
            dst_ref=v_att.at[pl.ds(i * chunk, chunk), own_cols],
            send_sem=att_ss.at[i],
            recv_sem=att_rs.at[i],
            device_id=(st, other),
            device_id_type=MESH,
        )

    n_chunks = rows_tok // chunk

    def attend_chunk(i, carry):
        per = n_blocks // n_chunks
        for k in range(per):
            attend(i * per + k)
        att_copy(i).start()
        return carry

    lax.fori_loop(0, n_chunks, attend_chunk, 0)


    def out_copy(i):
        at = pl.ds(i * chunk, chunk)
        return pltpu.make_async_copy(v_out.at[at], out.at[at], out_sem.at[i])

    def project(i, carry):
        at = pl.ds(pl.multiple_of(i * chunk, chunk), chunk)
        att_copy(i).wait_recv()
        cross = jnp.dot(v_att[at, :], v_wout[...], preferred_element_type=F32)
        v_out[at, :] = (v_conv[at, :] + jax.nn.sigmoid(gate_logit[...]) * cross).astype(BF)
        out_copy(i).start()
        return carry

    lax.fori_loop(0, n_chunks, project, 0)

    for i in range(n_chunks):
        out_copy(i).wait()
        att_copy(i).wait_send()


def settle_kernel(mixed, out, held, sems):
    pieces = sems.shape[1]
    rows = mixed.shape[0] // pieces

    def copies(i):
        at = pl.ds(i * rows, rows)
        return (
            pltpu.make_async_copy(mixed.at[at], held.at[at], sems.at[0, i]),
            pltpu.make_async_copy(held.at[at], out.at[at], sems.at[1, i]),
        )

    for i in range(pieces):
        copies(i)[0].start()
    for i in range(pieces):
        copies(i)[0].wait()
        copies(i)[1].start()
    for i in range(pieces):
        copies(i)[1].wait()


def on_device(
    tokens,
    norm_gain,
    branch_outer,
    branch_gate,
    branch_input,
    conv_taps,
    query_weight,
    query_gain,
    head_scale,
    store,
    store_gain,
    key_weight,
    value_weight,
    key_gain,
    out_weight,
    gate_logit,
    passage_ids,
):
    n_pass, plen, width = store.shape
    n_tok, half = tokens.shape
    heads = head_scale.shape[0]
    n_st = lax.axis_size("st")
    blocks = passage_ids.shape[0]

    vmem = pl.BlockSpec(memory_space=pltpu.VMEM)
    smem = pl.BlockSpec(memory_space=pltpu.SMEM)
    hbm = pl.BlockSpec(memory_space=pl.ANY)
    dma = pltpu.SemaphoreType.DMA
    scratch = [
        pltpu.VMEM((n_pass * plen, width), BF),
        pltpu.VMEM((width, 2 * HD), BF),
        pltpu.VMEM((256, width), BF),
        pltpu.VMEM((2, n_tok, half), BF),
        pltpu.VMEM((n_tok, width), BF),
        pltpu.VMEM(branch_outer.shape, BF),
        pltpu.VMEM(branch_gate.shape, BF),
        pltpu.VMEM(branch_input.shape, BF),
        pltpu.VMEM(query_weight.shape, BF),
        pltpu.VMEM(out_weight.shape, BF),
        pltpu.VMEM((blocks, heads, plen, HD), BF),
        pltpu.VMEM((n_tok, half), F32),
        pltpu.VMEM((n_tok, 2 * heads * HD), BF),
        pltpu.VMEM((n_tok, half), BF),
        pltpu.VMEM((3, RING, RING, 1, n_st * CAP), jnp.int32),
        pltpu.SMEM((3, RING, 1, n_st * CAP), jnp.int32),
        pltpu.SMEM((3, RING, RING, 1, n_st * CAP), jnp.int32),
        pltpu.VMEM((n_st * CAP, n_st * CAP), jnp.int32),
        pltpu.VMEM((3, 1, n_st * CAP), jnp.int32),
        pltpu.SMEM((3, 1, n_st * CAP), jnp.int32),
    ]
    for f in range(3):
        scratch += [pltpu.VMEM((n_pass, ROWS[f], HD), BF)] * RING
    for f in range(3):
        scratch += [pltpu.VMEM((RING, RING, len(g) * CAP, ROWS[f], HD), BF) for g in GROUP]
    for f in range(3):
        scratch += [pltpu.VMEM((RING, 3 * len(g) * CAP, ROWS[f], HD), BF) for g in GROUP]
    for f in range(3):
        scratch += [pltpu.VMEM((n_st * CAP, ROWS[f], HD), BF)]
    scratch += [
        dma((11,)),
        dma((4,)),
        dma((4,)),
        dma((3, 6)),
        dma((3, 6)),
        dma,
        dma,
        dma((9, 4)),
        dma((9, 4)),
        dma((27,)),
        dma((27,)),
        dma((81,)),
        dma((81,)),
        dma((4,)),
        dma((4,)),
    ]
    mixed = pl.pallas_call(
        kernel,
        out_shape=jax.ShapeDtypeStruct((n_tok, half), BF),
        in_specs=[
            smem,
            hbm,
            vmem,
            hbm,
            hbm,
            hbm,
            vmem,
            hbm,
            vmem,
            smem,
            hbm,
            vmem,
            hbm,
            hbm,
            vmem,
            hbm,
            vmem,
        ],
        out_specs=hbm,
        scratch_shapes=scratch,
        compiler_params=pltpu.CompilerParams(
            collective_id=0, has_side_effects=True, vmem_limit_bytes=56 * 1024 * 1024
        ),
    )(
        passage_ids.T,
        tokens,
        norm_gain.reshape(1, -1),
        branch_outer,
        branch_gate,
        branch_input,
        conv_taps,
        query_weight,
        query_gain.reshape(1, -1),
        head_scale,
        store.reshape(n_pass * plen, width),
        store_gain.reshape(1, -1),
        key_weight,
        value_weight,
        key_gain.reshape(1, -1),
        out_weight,
        gate_logit.reshape(1, -1),
    )
    pieces = 8
    return pl.pallas_call(
        settle_kernel,
        out_shape=jax.ShapeDtypeStruct((n_tok, half), BF),
        in_specs=[hbm],
        out_specs=hbm,
        scratch_shapes=[pltpu.VMEM((n_tok, half), BF), dma((2, pieces))],
        compiler_params=pltpu.CompilerParams(vmem_limit_bytes=62 * 1024 * 1024),
    )(mixed)


def solution(mesh):
    return jax.shard_map(
        on_device,
        mesh=mesh,
        in_specs=(
            P("st", "tp"),
            P(),
            P(None, "tp"),
            P(None, "tp"),
            P(None, "tp"),
            P(None, "tp"),
            P(None, "tp"),
            P(),
            P("tp"),
            P("st", None, None),
            P(),
            P(None, "tp"),
            P(None, "tp"),
            P(),
            P(None, "tp"),
            P("tp"),
            P("st", None),
        ),
        out_specs=P("st", "tp"),
        check_vma=False,
    )
```
